128 devices in a mesh: sp: 16 (over z, x), tp: 8 (over y, core).
Axes of the slice: x: 4, y: 4, z: 4, core: 2. Of those that a mesh axis runs over, the one named last changes fastest.
Arguments:
- queries: bfloat16 [16384, 1024], P('sp', 'tp'), may hold values from -6 to 6, as said below
- key_rows: bfloat16 [16384, 1024], P('sp', 'tp'), may hold values from -6 to 6, as said below
- value_rows: bfloat16 [16384, 1024], P('sp', 'tp'), may hold values from -6 to 6
- lambdas: float32 [8], P('tp'), may hold values from 0.3 to 0.8
- head_gain: float32 [128], replicated, may hold values from 0.1 to 1.9
- out_weight: bfloat16 [1024, 2048], replicated, may hold values from -0.1875 to 0.1875
- stream: bfloat16 [16384, 2048], P(('sp', 'tp')), may hold values from -6 to 6
- ffn_gain: float32 [2048], replicated, may hold values from 0.1 to 1.9
- routes: int32 [16384, 2], P(('sp', 'tp')), may hold values from 0 to 15, all different within a row; in each aligned block of 128 rows (0 to 127, 128 to 255, ...) at most 20 rows name the same one
- route_weight: float32 [16384, 2], P(('sp', 'tp')), may hold values from 0.1 to 1
- gate_weight: bfloat16 [16, 2048, 5120], P('sp', None, 'tp'), may hold values from -0.125 to 0.125
- up_weight: bfloat16 [16, 2048, 5120], P('sp', None, 'tp'), may hold values from -0.125 to 0.125
- down_weight: bfloat16 [16, 5120, 2048], P('sp', 'tp'), may hold values from -0.078125 to 0.078125
Outputs:
- layer_out: bfloat16 [16384, 2048], P(('sp', 'tp'))
The draws below stay inside these ranges and needn't reach their ends.
Inputs may be any that keep to these rules, and one draw needn't show every extreme that they name: Custom draw; the queries of a position meet only keys of the same or earlier positions. `key_rows`: custom draw. `routes`: each row names 2 different experts. In the 128 rows of one device no expert is named by more than 20 rows, and every draw reaches 20 on some device.
All inputs are finite; a program needn't handle non-finite values.
Results may differ from the reference program's by a relative error of at most 0.01.
Values may be sent and summed in bfloat16 or wider, within the bound.
No kernel may reach another device: no remote copies, remote signals or barrier semaphores. Data moves between devices by JAX's collectives and lax.ppermute only.
A program may use at most 128 MiB of HBM per device.

```python
import math
import jax
import jax.numpy as jnp
import numpy as np
from jax import lax

D = 2048
HEADS = 8
DH = 64
FE = 5120
TOPK = 2
TOKENS = 16384
TOK_POST = 128
EXPERTS = 16
SLOTS = 20
N_TP = 8


def draw_pair(key):
    width = HEADS * 2 * DH
    base_query = jax.random.fold_in(key, 101)
    base_key = jax.random.fold_in(key, 202)
    query_part = jnp.clip(1.3 * jax.random.normal(base_query, (TOKENS, width), jnp.float32), -6.0, 6.0)
    key_part = jnp.clip(1.3 * jax.random.normal(base_key, (TOKENS, width), jnp.float32), -6.0, 6.0)
    return (query_part, key_part)


def draw_queries(key, part):
    return draw_pair(key)[0].astype(jnp.bfloat16)


def draw_key_rows(key, part):
    return draw_pair(key)[1].astype(jnp.bfloat16)


def block_levels(stream_key, dims, split, least, high):
    def one(axis_at, blocks):
        draws = jax.random.uniform(jax.random.fold_in(jax.random.fold_in(stream_key, 6), axis_at), (blocks,), jnp.float32, least / len(split), high / len(split))
        return jnp.repeat(jnp.exp(draws), dims[axis_at] // blocks).reshape((-1,) + (1,) * (len(dims) - axis_at - 1))

    loudness = one(*split[0])
    for cut in split[1:]:
        loudness = loudness * one(*cut)
    return loudness


def deal_out(own_key, own, number, rows, number_of, top, bound, slope):
    sequence = jax.random.permutation(own_key, number_of)
    packed, ordinary = load_shares(number_of, rows * top, bound, slope, True), load_shares(number_of, rows * top, bound, slope, False)
    places = jnp.arange(number_of)

    def named(tallies, offset_by):
        used = int((tallies > 0).sum())
        fixed = max(1, used // 4)
        passed = fixed + (places - fixed + offset_by * (used - fixed)) % max(1, number_of - fixed)
        return jnp.zeros((number_of,), jnp.int32).at[sequence[jnp.where(places < fixed, places, passed)]].set(jnp.asarray(tallies, jnp.int32))

    tallies = jnp.where(number % 4 == 0, named(packed, number // 4), named(ordinary, number - number // 4 - 1))
    mixed = jax.random.permutation(jax.random.fold_in(own, 3), number_of)
    donor, taker = mixed[0:number_of // 2 * 2:2], mixed[1:number_of // 2 * 2:2]
    margin = jnp.minimum(tallies[donor] - 1, bound - tallies[taker]) // 2
    margin = jnp.where((donor == sequence[0]) | (taker == sequence[0]) | (tallies[taker] == 0), 0, jnp.maximum(margin, 0))
    passed = jax.random.randint(jax.random.fold_in(own, 4), (number_of // 2,), 0, 1 << 20) % (margin + 1)
    tallies = tallies.at[donor].add(-passed).at[taker].add(passed)
    members = jnp.searchsorted(jnp.cumsum(tallies), jnp.arange(rows * top), side="right").astype(jnp.int32)
    listing = members.reshape(top, rows).T
    listing = listing[jax.random.permutation(jax.random.fold_in(own, 1), rows)]
    offset_by = jax.random.randint(jax.random.fold_in(own, 2), (rows, 1), 0, top)
    return jnp.take_along_axis(listing, (jnp.arange(top)[None, :] + offset_by) % top, axis=1)


def load_shares(amount, total, bound, lean, full):
    portions = [(1 << 20) // math.isqrt(grade ** lean) + 1 for grade in range(1, amount + 1)]
    largest = bound if full else min(bound, max(-(-total // amount), total * portions[0] // sum(portions)))
    least = 1 if total - largest >= amount - 1 else 0
    counts, surplus = [largest] + [least] * (amount - 1), total - largest - least * (amount - 1)
    while surplus > 0:
        free = [i for i in range(1, amount) if counts[i] < largest] or [i for i in range(1, amount) if counts[i] < bound]
        pool, budget = sum([portions[i] for i in free]), surplus
        for i in free:
            addition = min(bound - counts[i], max(1, budget * portions[i] // pool), surplus)
            counts[i] = counts[i] + addition
            surplus = surplus - addition
    return np.array(counts)


def normal_values(rng, dims, scale, limit, pieces=(), kind=jnp.bfloat16):
    entries = jax.random.normal(rng, dims, jnp.float32) * scale
    if len(pieces) > 0:
        entries = block_levels(rng, dims, pieces, -0.22, 0.18) * entries
    return jnp.clip(entries, min=-limit, max=limit).astype(kind)


def setup_inputs(seed: int = 0) -> dict:
    streams_of = jax.random.split(jax.random.key(seed), 14)
    queries = draw_queries(jax.random.fold_in(streams_of[13], 71), 0)
    key_rows = draw_key_rows(jax.random.fold_in(streams_of[13], 71), 0)
    value_rows = normal_values(streams_of[2], (TOKENS, HEADS * 2 * DH), 1.0, 6.0, ((0, 16), (1, 8)))
    lambdas = jnp.clip(0.3 + 0.5 * jax.random.uniform(streams_of[3], (HEADS,), jnp.float32) ** block_levels(streams_of[3], (HEADS,), ((0, 8),), -0.2, 0.2), 0.3, 0.8)
    head_gain = jnp.clip(1.0 + 0.18 * jax.random.normal(streams_of[4], (2 * DH,), jnp.float32), 0.1, 1.9)
    out_weight = normal_values(streams_of[5], (HEADS * 2 * DH, D), (HEADS * 2 * DH) ** -0.5, 0.1875)
    stream = normal_values(streams_of[6], (TOKENS, D), 1.0, 6.0, ((0, 128),))
    ffn_gain = jnp.clip(1.0 + 0.18 * jax.random.normal(streams_of[7], (D,), jnp.float32), 0.1, 1.9)
    routes_keys = jax.random.split(jax.random.fold_in(streams_of[8], 1), TOKENS // TOK_POST)
    routes_turns = jax.random.permutation(jax.random.fold_in(streams_of[8], 3), TOKENS // TOK_POST)
    routes = jax.vmap(lambda own, number: deal_out(jax.random.fold_in(streams_of[8], 2), own, number, TOK_POST, EXPERTS, TOPK, SLOTS, 1))(routes_keys, routes_turns).reshape((TOKENS, TOPK))
    route_weight = jnp.clip(0.1 + 0.9 * jax.random.uniform(streams_of[9], (TOKENS, TOPK), jnp.float32) ** block_levels(streams_of[9], (TOKENS, TOPK), ((0, 128),), -0.2, 0.2), 0.1, 1.0)
    gate_weight = normal_values(streams_of[10], (EXPERTS, D, FE), D ** -0.5, 0.125, ((0, 16), (2, 8)))
    up_weight = normal_values(streams_of[11], (EXPERTS, D, FE), D ** -0.5, 0.125, ((0, 16), (2, 8)))
    down_weight = normal_values(streams_of[12], (EXPERTS, FE, D), FE ** -0.5, 0.078125, ((0, 16), (1, 8)))
    return dict(queries=queries, key_rows=key_rows, value_rows=value_rows, lambdas=lambdas, head_gain=head_gain, out_weight=out_weight, stream=stream, ffn_gain=ffn_gain, routes=routes, route_weight=route_weight, gate_weight=gate_weight, up_weight=up_weight, down_weight=down_weight)


def attention(queries, key_rows, value_rows, lambdas, head_gain):
    tokens = queries.shape[0]
    q_all = queries.astype(jnp.float32).reshape(tokens, HEADS, 2, DH)
    k_all = key_rows.astype(jnp.float32).reshape(tokens, HEADS, 2, DH)
    v_all = value_rows.astype(jnp.float32).reshape(tokens, HEADS, 2 * DH)
    block = math.gcd(tokens, 256)
    key_pos = jnp.arange(tokens, dtype=jnp.int32)

    def attend(start):
        q_block = lax.dynamic_slice_in_dim(q_all, start, block, 0)
        scores = jnp.einsum('qhmd,khmd->hmqk', q_block, k_all) * DH ** (-0.5)
        query_pos = start + jnp.arange(block, dtype=jnp.int32)
        mask = key_pos[None, :] <= query_pos[:, None]
        scores = jnp.where(mask, scores, -jnp.inf)
        top = lax.optimization_barrier(jnp.max(scores, axis=-1, keepdims=True))
        expo = jnp.exp(scores - top)
        total = lax.optimization_barrier(jnp.sum(expo, axis=-1))
        weights = lax.optimization_barrier(expo.astype(jnp.bfloat16)).astype(jnp.float32)
        mixed = jnp.einsum('hmqk,khe->hmqe', weights, v_all) / total[..., None]
        contrast = mixed[:, 0] - lambdas[:, None, None] * mixed[:, 1]
        contrast = contrast * lax.rsqrt(lax.optimization_barrier(jnp.mean(contrast * contrast, axis=-1, keepdims=True)) + 1e-05) * head_gain
        return jnp.transpose(contrast, (1, 0, 2)).reshape(block, HEADS * 2 * DH).astype(jnp.bfloat16)
    starts = jnp.arange(tokens // block, dtype=jnp.int32) * block
    return lax.map(attend, starts).reshape(tokens, HEADS * 2 * DH)

def reference(queries, key_rows, value_rows, lambdas, head_gain, out_weight, stream, ffn_gain, routes, route_weight, gate_weight, up_weight, down_weight):
    tokens = queries.shape[0]
    heads_out = attention(queries, key_rows, value_rows, lambdas, head_gain)
    attended = stream.astype(jnp.float32) + jnp.dot(heads_out, out_weight, preferred_element_type=jnp.float32)
    normed = (attended * lax.rsqrt(lax.optimization_barrier(jnp.mean(attended * attended, axis=-1, keepdims=True)) + 1e-06) * ffn_gain).astype(jnp.bfloat16)
    capacity = tokens // TOK_POST * SLOTS

    def expert(carry, index):
        hits = routes == index
        weight = lax.optimization_barrier(jnp.sum(jnp.where(hits, route_weight, 0.0), axis=1))
        chosen = jnp.any(hits, axis=1)
        count = jnp.sum(chosen.astype(jnp.int32))
        picked = jnp.nonzero(chosen, size=capacity, fill_value=0)[0].astype(jnp.int32)
        rows = normed[picked]
        gate = jnp.dot(rows, gate_weight[index], preferred_element_type=jnp.float32)
        upper = jnp.dot(rows, up_weight[index], preferred_element_type=jnp.float32)
        act = (jax.nn.silu(gate) * upper).astype(jnp.bfloat16)
        parts = jnp.einsum('rcf,cfd->rcd', act.astype(jnp.float32).reshape(capacity, N_TP, FE // N_TP), down_weight[index].astype(jnp.float32).reshape(N_TP, FE // N_TP, D))
        parts = lax.optimization_barrier(parts.astype(jnp.bfloat16)).astype(jnp.float32)
        summed = lax.optimization_barrier(lax.optimization_barrier(jnp.sum(parts, axis=1)).astype(jnp.bfloat16)).astype(jnp.float32)
        valid = jnp.arange(capacity, dtype=jnp.int32) < count
        scale = jnp.where(valid, weight[picked], 0.0)
        return (carry.at[picked].add(summed * scale[:, None]), None)
    start = jnp.zeros((tokens, D), jnp.float32)
    routed, _ = lax.scan(expert, start, jnp.arange(EXPERTS, dtype=jnp.int32))
    return (attended + routed).astype(jnp.bfloat16)
```

```python
import math

import jax
import jax.numpy as jnp
from jax import lax
from jax.experimental import pallas as pl
from jax.experimental.pallas import tpu as pltpu
from jax.sharding import PartitionSpec as P

DH = 64
KEYS = 1024
ROWS = 256
SCALE = DH**-0.5 * math.log2(math.e)
BOTH = ("sp", "tp")
F32 = jnp.float32
BF16 = jnp.bfloat16
VMEM_LIMIT = 56 * 1024 * 1024


def dot(a, b, dims=((1,), (0,))):
    return lax.dot_general(a, b, (dims, ((), ())), preferred_element_type=F32)


def attention_body(half_at, key_at, pos_at, out_at, q_ref, k_ref, v_ref, lam_ref, gain_ref, o_ref, m_sc, acc_sc):
    step = pl.program_id(0)
    begin = key_at[step] * KEYS
    q_pos = pos_at[step]
    rows = q_ref.shape[2]

    @pl.when(begin == 0)
    def _():
        m_sc[...] = jnp.full(m_sc.shape, -1e30, F32)
        acc_sc[...] = jnp.zeros(acc_sc.shape, F32)

    last = begin + KEYS > q_pos

    def run(masked):
        k = k_ref[...]
        v = jnp.concatenate([v_ref[...], jnp.ones((KEYS, 128), BF16)], axis=1)
        tiles = [(m, r) for r in range(rows // ROWS) for m in range(2)]

        def scores(m, r):
            s = dot(q_ref[0, m, pl.ds(r * ROWS, ROWS), :], k, ((1,), (1,)))
            if masked:
                row = r * ROWS + lax.broadcasted_iota(jnp.int32, s.shape, 0)
                at = q_pos + lax.shift_right_logical(row, 6) * 128 + (row & 63)
                key = begin + lax.broadcasted_iota(jnp.int32, s.shape, 1)
                s = jnp.where(key <= at, s, -1e30)
            return s

        def finish(m, r, s):
            at = pl.ds(r * ROWS, ROWS)
            old = m_sc[m, at, :]
            new = jnp.maximum(old, jnp.max(s, axis=1, keepdims=True))
            m_sc[m, at, :] = new
            p = jnp.exp2((s - jnp.concatenate([new] * (KEYS // 128), axis=1)) * SCALE)
            factor = jnp.exp2((old - new) * SCALE)
            both = jnp.concatenate([factor, factor], axis=1)
            acc_sc[m, at, :] = acc_sc[m, at, :] * both + dot(p.astype(BF16), v)

        s = scores(*tiles[0])
        for n, tile in enumerate(tiles):
            after = scores(*tiles[n + 1]) if n + 1 < len(tiles) else None
            finish(*tile, s)
            s = after

    @pl.when(jnp.logical_not(last))
    def _():
        run(False)

    @pl.when(last)
    def _():
        run(True)
        first = acc_sc[0, :, :128] / acc_sc[0, :, 128:]
        second = acc_sc[1, :, :128] / acc_sc[1, :, 128:]
        c = first - lam_ref[0] * second
        c = c * lax.rsqrt(jnp.mean(c * c, axis=1, keepdims=True) + 1e-05) * gain_ref[...]
        o_ref[0] = c.astype(BF16)


def attention(own, other, kv, lambdas, gain, sp, sp_size):
    half = own.shape[0]
    zero = jnp.zeros((2, half, DH), BF16)
    q = jnp.stack([other, own])
    q = jnp.stack(
        [
            jnp.concatenate([q[..., :DH], zero], -1),
            jnp.concatenate([zero, q[..., DH:]], -1),
        ],
        1,
    )
    steps = sp_size + 1
    step = jnp.arange(steps, dtype=jnp.int32)
    count = sp_size - sp
    is_other = step < count
    low = sp < sp_size // 2
    half_at = jnp.where(is_other, 0, 1).astype(jnp.int32)
    key_at = jnp.where(is_other, step, step - count).astype(jnp.int32)
    pos_at = jnp.where(is_other, (sp_size - 1 - sp) * KEYS + 64, sp * KEYS).astype(jnp.int32)
    out_at = jnp.where(is_other == low, 1, 0).astype(jnp.int32)
    spec = pltpu.PrefetchScalarGridSpec(
        num_scalar_prefetch=4,
        grid=(steps,),
        in_specs=[
            pl.BlockSpec((1, 2, half, 128), lambda s, h, k, p, o: (h[s], 0, 0, 0)),
            pl.BlockSpec((KEYS, 128), lambda s, h, k, p, o: (k[s], 0)),
            pl.BlockSpec((KEYS, 128), lambda s, h, k, p, o: (k[s], 1)),
            pl.BlockSpec(memory_space=pltpu.SMEM),
            pl.BlockSpec((1, 128), lambda s, h, k, p, o: (0, 0)),
        ],
        out_specs=pl.BlockSpec((1, half, 128), lambda s, h, k, p, o: (o[s], 0, 0)),
        scratch_shapes=[pltpu.VMEM((2, half, 128), F32), pltpu.VMEM((2, half, 256), F32)],
    )
    return pl.pallas_call(
        attention_body,
        grid_spec=spec,
        out_shape=jax.ShapeDtypeStruct((2, half, 128), BF16),
        compiler_params=pltpu.CompilerParams(
            dimension_semantics=("arbitrary",), vmem_limit_bytes=VMEM_LIMIT
        ),
        name="attention",
    )(half_at, key_at, pos_at, out_at, q, kv, kv, lambdas, gain.reshape(1, 128))


def project_body(h_ref, w_ref, s_ref, g_ref, d_ref, a_ref, o_ref):
    parts = [jnp.concatenate([h_ref[n, t] for t in range(h_ref.shape[1])], axis=1) for n in range(2)]
    x = jnp.concatenate(parts, axis=0)
    attended = s_ref[...].astype(F32) + dot(x, w_ref[...])
    a_ref[...] = attended
    mean = jnp.mean(attended * attended, axis=1, keepdims=True)
    normed = (attended * lax.rsqrt(mean + 1e-06) * g_ref[...]).astype(BF16)
    wide = normed.shape[1] // 2
    o_ref[...] = (dot(d_ref[0], normed[:, :wide]) + dot(d_ref[1], normed[:, wide:])).astype(BF16)


def project(heads, out_weight, stream, gain, dispatch):
    rows, width = stream.shape
    return pl.pallas_call(
        project_body,
        out_shape=(
            jax.ShapeDtypeStruct((rows, width), F32),
            jax.ShapeDtypeStruct((dispatch.shape[1], width // 2), BF16),
        ),
        compiler_params=pltpu.CompilerParams(vmem_limit_bytes=VMEM_LIMIT),
        name="project",
    )(heads, out_weight, stream, gain.reshape(1, width), dispatch)


def expert_body(sets, r_ref, s_ref, *refs):
    weights, (o_ref, x_sc, acc_sc, g_buf, u_buf, d_buf, sem) = refs[: 3 * sets], refs[3 * sets :]
    buffers = (g_buf, u_buf, d_buf)

    def copy(n, kind):
        return pltpu.make_async_copy(weights[3 * n + kind], buffers[kind].at[n % 2], sem.at[n % 2, kind])

    for kind in range(3):
        copy(0, kind).start()
    wide = r_ref.shape[1]
    x_sc[:, :wide] = dot(s_ref[0], r_ref[...]).astype(BF16)
    x_sc[:, wide:] = dot(s_ref[1], r_ref[...]).astype(BF16)
    x = x_sc[...]
    for n in range(sets):
        if n + 1 < sets:
            for kind in range(3):
                copy(n + 1, kind).start()
        copy(n, 0).wait()
        gate = dot(x, g_buf[n % 2])
        copy(n, 1).wait()
        upper = dot(x, u_buf[n % 2])
        act = (gate / (1.0 + jnp.exp(-gate)) * upper).astype(BF16)
        copy(n, 2).wait()
        part = dot(act, d_buf[n % 2])
        if n == 0:
            acc_sc[...] = part
        elif n + 1 < sets:
            acc_sc[...] += part
        else:
            o_ref[...] = (acc_sc[...] + part).astype(o_ref.dtype)


def expert(arrived, select, sets, dtype):
    rows = select.shape[1]
    width, hidden = sets[0][0].shape
    flat = [w for one in sets for w in one]
    whole = pl.BlockSpec(memory_space=pltpu.VMEM)
    return pl.pallas_call(
        lambda *refs: expert_body(len(sets), *refs),
        in_specs=[whole, whole] + [pl.BlockSpec(memory_space=pl.ANY)] * len(flat),
        out_specs=whole,
        out_shape=jax.ShapeDtypeStruct((rows, width), dtype),
        scratch_shapes=[
            pltpu.VMEM((rows, width), BF16),
            pltpu.VMEM((rows, width), F32),
            pltpu.VMEM((2, width, hidden), BF16),
            pltpu.VMEM((2, width, hidden), BF16),
            pltpu.VMEM((2, hidden, width), BF16),
            pltpu.SemaphoreType.DMA((2, 3)),
        ],
        compiler_params=pltpu.CompilerParams(vmem_limit_bytes=VMEM_LIMIT),
        name="expert",
    )(arrived, select, *flat)


def pack_body(a_ref, b_ref, s_ref, o_ref):
    total = (a_ref[...] + b_ref[...].astype(F32)).astype(BF16)
    wide = total.shape[1] // 2
    o_ref[...] = (
        dot(s_ref[0], total[:, :wide], ((0,), (0,))) + dot(s_ref[1], total[:, wide:], ((0,), (0,)))
    ).astype(BF16)


def pack(mine, theirs, select):
    return pl.pallas_call(
        pack_body,
        out_shape=jax.ShapeDtypeStruct((select.shape[2], mine.shape[1] // 2), BF16),
        compiler_params=pltpu.CompilerParams(vmem_limit_bytes=VMEM_LIMIT),
        name="pack",
    )(mine, theirs, select)


def combine_body(r_ref, high_ref, low_ref, a_ref, o_ref):
    r = r_ref[...]
    wide = r.shape[1]
    for n in range(2):
        at = slice(n * wide, n * wide + wide)
        routed = dot(high_ref[n], r) + dot(low_ref[n], r)
        o_ref[:, at] = (a_ref[:, at] + routed).astype(BF16)


def combine(returned, high, low, attended):
    return pl.pallas_call(
        combine_body,
        out_shape=jax.ShapeDtypeStruct(attended.shape, BF16),
        compiler_params=pltpu.CompilerParams(vmem_limit_bytes=VMEM_LIMIT),
        name="combine",
    )(returned, high, low, attended)


def moved(sp_size, tp_size, shift, flip):
    pairs = []
    for s in range(sp_size):
        for t in range(tp_size):
            y, c = t // 2, t % 2
            to = (y + shift(c)) % (tp_size // 2) * 2 + (c ^ flip)
            pairs.append((s * tp_size + t, s * tp_size + to))
    return pairs


def local(
    queries,
    key_rows,
    value_rows,
    lambdas,
    head_gain,
    out_weight,
    stream,
    ffn_gain,
    routes,
    route_weight,
    gate_weight,
    up_weight,
    down_weight,
):
    sp_size = lax.axis_size("sp")
    tp_size = lax.axis_size("tp")
    sp = lax.axis_index("sp")
    length = queries.shape[0]
    rows_local, width = stream.shape
    experts = sp_size * gate_weight.shape[0]
    top_count = routes.shape[1]
    low = sp < sp_size // 2

    kv = lax.all_gather(jnp.concatenate([key_rows, value_rows], axis=1), "sp", axis=0, tiled=True)
    split = queries.reshape(tp_size, 2, length // (2 * tp_size), queries.shape[1])
    own = split[:, 0].reshape(length // 2, -1)
    other = lax.ppermute(
        split[:, 1].reshape(length // 2, -1), "sp", [(s, sp_size - 1 - s) for s in range(sp_size)]
    )

    mine = (gate_weight[0], up_weight[0], down_weight[0])
    along = moved(sp_size, tp_size, lambda c: 2 * c - 1, 0)
    sibling = moved(sp_size, tp_size, lambda c: 0, 1)
    opposite = moved(sp_size, tp_size, lambda c: tp_size // 4, 0)
    passed = tuple(lax.ppermute(w, BOTH, along) for w in mine)
    mine_too = tuple(lax.ppermute(w, BOTH, sibling) for w in mine)
    passed_too = tuple(lax.ppermute(w, BOTH, sibling) for w in passed)
    sets = (mine, mine_too, passed, passed_too)

    slots = max(2, (rows_local * top_count * 5 + 4 * experts - 1) // (4 * experts))
    flat = routes.reshape(-1)
    onehot = (flat[:, None] == jnp.arange(experts, dtype=jnp.int32)[None, :]).astype(BF16)
    count = flat.shape[0]
    earlier = (jnp.arange(count)[None, :] < jnp.arange(count)[:, None]).astype(BF16)
    slot = jnp.sum(dot(earlier, onehot) * onehot.astype(F32), axis=1).astype(jnp.int32)
    at = (flat * (2 * slots) + slot).reshape(rows_local, top_count)
    packed = experts * slots * 2
    places = jnp.arange(packed, dtype=jnp.int32)
    hits = [[at[:, k] + n * slots for k in range(top_count)] for n in range(2)]
    dispatch = jnp.stack(
        [sum((places[:, None] == h[None, :]).astype(F32) for h in hits[n]) for n in range(2)]
    ).astype(BF16)
    weighted = jnp.stack(
        [
            sum(
                jnp.where(places[None, :] == h[:, None], route_weight[:, k : k + 1], 0.0)
                for k, h in enumerate(hits[n])
            )
            for n in range(2)
        ]
    )
    high = weighted.astype(BF16)
    low_part = (weighted - lax.reduce_precision(weighted, 8, 7)).astype(BF16)
    row = jnp.arange(experts * slots, dtype=jnp.int32)
    packed_row = row // slots * (2 * slots) + row % slots
    select = jnp.stack(
        [(packed_row[:, None] + n * slots == places[None, :]).astype(BF16) for n in range(2)]
    )

    heads = attention(own, other, kv, lambdas, head_gain, sp, sp_size)
    half = rows_local // 2
    heads = heads.reshape(2 * tp_size, half, 128)
    groups = [
        [s * tp_size + t for s in (n, sp_size - 1 - n) for t in range(tp_size)]
        for n in range(sp_size // 2)
    ]
    heads = lax.all_to_all(
        heads, BOTH, split_axis=0, concat_axis=0, tiled=True, axis_index_groups=groups
    ).reshape(2, tp_size, half, 128)
    heads = jnp.where(low, heads, heads[::-1])

    attended, outgoing = project(heads, out_weight, stream, ffn_gain, dispatch)
    arrived = lax.all_to_all(
        outgoing.reshape(experts, 2 * slots, width // 2), "sp", split_axis=0, concat_axis=0, tiled=True
    ).reshape(packed, width // 2)
    theirs = lax.ppermute(arrived, BOTH, opposite)
    kept = expert(arrived, select, sets, F32)
    given = expert(theirs, select, sets, BF16)
    got = lax.ppermute(given, BOTH, opposite)
    returned = lax.all_to_all(
        pack(kept, got, select).reshape(experts, 2 * slots, width // 2),
        "sp",
        split_axis=0,
        concat_axis=0,
        tiled=True,
    ).reshape(packed, width // 2)
    return combine(returned, high, low_part, attended)


def solution(mesh):
    placed = (
        P("sp", "tp"),
        P("sp", "tp"),
        P("sp", "tp"),
        P("tp"),
        P(),
        P(),
        P(("sp", "tp"), None),
        P(),
        P(("sp", "tp"), None),
        P(("sp", "tp"), None),
        P("sp", None, "tp"),
        P("sp", None, "tp"),
        P("sp", "tp", None),
    )
    return jax.shard_map(
        local, mesh=mesh, in_specs=placed, out_specs=P(("sp", "tp"), None), check_vma=False
    )
```

```python
import math

import jax
import jax.numpy as jnp
from jax import lax
from jax.experimental import pallas as pl
from jax.experimental.pallas import tpu as pltpu
from jax.sharding import PartitionSpec as P

DH = 64
KEYS = 1024
ROWS = 256
SCALE = DH**-0.5 * math.log2(math.e)
BOTH = ("sp", "tp")
F32 = jnp.float32
BF16 = jnp.bfloat16
VMEM_LIMIT = 58 * 1024 * 1024
CHUNKS = 2
CUTS = 4
FLOPS_US = 1.0e9


def dot(a, b, dims=((1,), (0,))):
    return lax.dot_general(a, b, (dims, ((), ())), preferred_element_type=F32)


def attention_body(half_at, key_at, pos_at, out_at, q_ref, k_ref, v_ref, lam_ref, gain_ref, o_ref, m_sc, acc_sc):
    step = pl.program_id(0)
    begin = key_at[step] * KEYS
    q_pos = pos_at[step]
    rows = q_ref.shape[2]

    @pl.when(begin == 0)
    def _():
        m_sc[...] = jnp.full(m_sc.shape, -1e30, F32)
        acc_sc[...] = jnp.zeros(acc_sc.shape, F32)

    last = begin + KEYS > q_pos

    def run(masked):
        k = k_ref[...]
        v = jnp.concatenate([v_ref[...], jnp.ones((KEYS, 128), BF16)], axis=1)
        tiles = [(m, r) for r in range(rows // ROWS) for m in range(2)]

        def scores(m, r):
            s = dot(q_ref[0, m, pl.ds(r * ROWS, ROWS), :], k, ((1,), (1,)))
            if masked:
                row = r * ROWS + lax.broadcasted_iota(jnp.int32, s.shape, 0)
                at = q_pos + lax.shift_right_logical(row, 6) * 128 + (row & 63)
                key = begin + lax.broadcasted_iota(jnp.int32, s.shape, 1)
                s = jnp.where(key <= at, s, -1e30)
            return s

        def finish(m, r, s):
            at = pl.ds(r * ROWS, ROWS)
            old = m_sc[m, at, :]
            new = jnp.maximum(old, jnp.max(s, axis=1, keepdims=True))
            m_sc[m, at, :] = new
            p = jnp.exp2((s - jnp.concatenate([new] * (KEYS // 128), axis=1)) * SCALE)
            factor = jnp.exp2((old - new) * SCALE)
            both = jnp.concatenate([factor, factor], axis=1)
            acc_sc[m, at, :] = acc_sc[m, at, :] * both + dot(p.astype(BF16), v)

        s = scores(*tiles[0])
        for n, tile in enumerate(tiles):
            after = scores(*tiles[n + 1]) if n + 1 < len(tiles) else None
            finish(*tile, s)
            s = after

    @pl.when(jnp.logical_not(last))
    def _():
        run(False)

    @pl.when(last)
    def _():
        run(True)
        first = acc_sc[0, :, :128] / acc_sc[0, :, 128:]
        second = acc_sc[1, :, :128] / acc_sc[1, :, 128:]
        c = first - lam_ref[0] * second
        c = c * lax.rsqrt(jnp.mean(c * c, axis=1, keepdims=True) + 1e-05) * gain_ref[...]
        o_ref[0] = c.astype(BF16)


def attention(own, other, kv, lambdas, gain, sp, sp_size):
    half = own.shape[0]
    zero = jnp.zeros((2, half, DH), BF16)
    q = jnp.stack([other, own])
    q = jnp.stack(
        [
            jnp.concatenate([q[..., :DH], zero], -1),
            jnp.concatenate([zero, q[..., DH:]], -1),
        ],
        1,
    )
    steps = sp_size + 1
    step = jnp.arange(steps, dtype=jnp.int32)
    count = sp_size - sp
    is_other = step < count
    low = sp < sp_size // 2
    half_at = jnp.where(is_other, 0, 1).astype(jnp.int32)
    key_at = jnp.where(is_other, step, step - count).astype(jnp.int32)
    pos_at = jnp.where(is_other, (sp_size - 1 - sp) * KEYS + 64, sp * KEYS).astype(jnp.int32)
    out_at = jnp.where(is_other == low, 1, 0).astype(jnp.int32)
    spec = pltpu.PrefetchScalarGridSpec(
        num_scalar_prefetch=4,
        grid=(steps,),
        in_specs=[
            pl.BlockSpec((1, 2, half, 128), lambda s, h, k, p, o: (h[s], 0, 0, 0)),
            pl.BlockSpec((KEYS, 128), lambda s, h, k, p, o: (k[s], 0)),
            pl.BlockSpec((KEYS, 128), lambda s, h, k, p, o: (k[s], 1)),
            pl.BlockSpec(memory_space=pltpu.SMEM),
            pl.BlockSpec((1, 128), lambda s, h, k, p, o: (0, 0)),
        ],
        out_specs=pl.BlockSpec((1, half, 128), lambda s, h, k, p, o: (o[s], 0, 0)),
        scratch_shapes=[pltpu.VMEM((2, half, 128), F32), pltpu.VMEM((2, half, 256), F32)],
    )
    return pl.pallas_call(
        attention_body,
        grid_spec=spec,
        out_shape=jax.ShapeDtypeStruct((2, half, 128), BF16),
        compiler_params=pltpu.CompilerParams(
            dimension_semantics=("arbitrary",), vmem_limit_bytes=VMEM_LIMIT
        ),
        cost_estimate=cost(29),
        name="attention",
    )(half_at, key_at, pos_at, out_at, q, kv, kv, lambdas, gain.reshape(1, 128))


def project_body(h_ref, w_ref, s_ref, g_ref, d_ref, a_ref, *o_refs):
    parts = [jnp.concatenate([h_ref[n, t] for t in range(h_ref.shape[1])], axis=1) for n in range(2)]
    x = jnp.concatenate(parts, axis=0)
    attended = s_ref[...].astype(F32) + dot(x, w_ref[...])
    a_ref[...] = attended
    mean = jnp.mean(attended * attended, axis=1, keepdims=True)
    normed = (attended * lax.rsqrt(mean + 1e-06) * g_ref[...]).astype(BF16)
    for c, o_ref in enumerate(o_refs):
        o_ref[...] = sum(dot(d_ref[c, n], cut(normed, n)) for n in range(CUTS)).astype(BF16)


def cut(x, n):
    wide = x.shape[1] // CUTS
    return x[:, n * wide : (n + 1) * wide]


def project(heads, out_weight, stream, gain, dispatch):
    rows, width = stream.shape
    packed = jax.ShapeDtypeStruct((dispatch.shape[2], width // CUTS), BF16)
    return pl.pallas_call(
        project_body,
        out_shape=(jax.ShapeDtypeStruct((rows, width), F32),) + (packed,) * CHUNKS,
        compiler_params=pltpu.CompilerParams(vmem_limit_bytes=VMEM_LIMIT),
        cost_estimate=cost(5),
        name="project",
    )(heads, out_weight, stream, gain.reshape(1, width), dispatch)


def cost(microseconds):
    return pl.CostEstimate(flops=int(microseconds * FLOPS_US), bytes_accessed=0, transcendentals=0)


def expert_body(chunks, sets, *refs):
    r_refs, s_ref, weights = refs[:chunks], refs[chunks], refs[chunks + 1 : chunks + 1 + 3 * sets]
    o_refs = refs[chunks + 1 + 3 * sets : 2 * chunks + 1 + 3 * sets]
    x_sc, acc_sc, in_buf, down_buf, sem = refs[2 * chunks + 1 + 3 * sets :]
    hidden = in_buf.shape[2] // 2
    rows = s_ref.shape[1]

    def copy(n, kind):
        if kind < 2:
            to = in_buf.at[n, :, pl.ds(kind * hidden, hidden)]
        else:
            to = down_buf.at[n // 2, pl.ds(n % 2 * hidden, hidden), :]
        return pltpu.make_async_copy(weights[3 * n + kind], to, sem.at[3 * n + kind])

    for p in range(sets // 2):
        for n, kind in ((0, 0), (0, 1), (1, 0), (1, 1), (0, 2), (1, 2)):
            copy(2 * p + n, kind).start()
    wide = r_refs[0].shape[1]
    for c in range(chunks):
        for n in range(CUTS):
            x_sc[c * rows : (c + 1) * rows, n * wide : (n + 1) * wide] = dot(
                s_ref[n], r_refs[c][...]
            ).astype(BF16)
    x = x_sc[...]
    for p in range(sets // 2):
        acts = []
        for n in (2 * p, 2 * p + 1):
            copy(n, 0).wait()
            copy(n, 1).wait()
            both = dot(x, in_buf[n])
            gate, upper = both[:, :hidden], both[:, hidden:]
            acts.append((gate / (1.0 + jnp.exp(-gate)) * upper).astype(BF16))
        copy(2 * p, 2).wait()
        copy(2 * p + 1, 2).wait()
        part = dot(jnp.concatenate(acts, axis=1), down_buf[p])
        if p == 0:
            acc_sc[...] = part
        elif p + 1 < sets // 2:
            acc_sc[...] += part
        else:
            whole = (acc_sc[...] + part).astype(o_refs[0].dtype)
            for c in range(chunks):
                o_refs[c][...] = whole[c * rows : (c + 1) * rows]


def expert(arrived, select, sets, dtype):
    chunks = len(arrived)
    rows = select.shape[1]
    width, hidden = sets[0][0].shape
    flat = [w for one in sets for w in one]
    whole = pl.BlockSpec(memory_space=pltpu.VMEM)
    return pl.pallas_call(
        lambda *refs: expert_body(chunks, len(sets), *refs),
        in_specs=[whole] * (chunks + 1) + [pl.BlockSpec(memory_space=pl.ANY)] * len(flat),
        out_specs=[whole] * chunks,
        out_shape=[jax.ShapeDtypeStruct((rows, width), dtype)] * chunks,
        scratch_shapes=[
            pltpu.VMEM((chunks * rows, width), BF16),
            pltpu.VMEM((chunks * rows, width), F32),
            pltpu.VMEM((len(sets), width, 2 * hidden), BF16),
            pltpu.VMEM((len(sets) // 2, 2 * hidden, width), BF16),
            pltpu.SemaphoreType.DMA((len(flat),)),
        ],
        compiler_params=pltpu.CompilerParams(vmem_limit_bytes=VMEM_LIMIT),
        cost_estimate=cost(6 + 4 * chunks),
        name="expert",
    )(*arrived, select, *flat)


def pack_body(a_ref, b_ref, s_ref, o_ref):
    total = (a_ref[...] + b_ref[...].astype(F32)).astype(BF16)
    o_ref[...] = sum(dot(s_ref[n], cut(total, n), ((0,), (0,))) for n in range(CUTS)).astype(BF16)


def pack(mine, theirs, select):
    return pl.pallas_call(
        pack_body,
        out_shape=jax.ShapeDtypeStruct((select.shape[2], mine.shape[1] // CUTS), BF16),
        compiler_params=pltpu.CompilerParams(vmem_limit_bytes=VMEM_LIMIT),
        cost_estimate=cost(2),
        name="pack",
    )(mine, theirs, select)


def combine_body(*refs):
    r_refs, (high_ref, low_ref, a_ref, o_ref) = refs[:CHUNKS], refs[CHUNKS:]
    wide = r_refs[0].shape[1]
    for n in range(CUTS):
        at = slice(n * wide, n * wide + wide)
        routed = a_ref[:, at]
        for c in range(CHUNKS):
            r = r_refs[c][...]
            routed = routed + dot(high_ref[c, n], r) + dot(low_ref[c, n], r)
        o_ref[:, at] = routed.astype(BF16)


def combine(returned, high, low, attended):
    return pl.pallas_call(
        combine_body,
        out_shape=jax.ShapeDtypeStruct(attended.shape, BF16),
        compiler_params=pltpu.CompilerParams(vmem_limit_bytes=VMEM_LIMIT),
        name="combine",
    )(*returned, high, low, attended)


def moved(sp_size, tp_size, shift, flip):
    pairs = []
    for s in range(sp_size):
        for t in range(tp_size):
            y, c = t // 2, t % 2
            to = (y + shift(c)) % (tp_size // 2) * 2 + (c ^ flip)
            pairs.append((s * tp_size + t, s * tp_size + to))
    return pairs


def local(
    queries,
    key_rows,
    value_rows,
    lambdas,
    head_gain,
    out_weight,
    stream,
    ffn_gain,
    routes,
    route_weight,
    gate_weight,
    up_weight,
    down_weight,
):
    sp_size = lax.axis_size("sp")
    tp_size = lax.axis_size("tp")
    sp = lax.axis_index("sp")
    length = queries.shape[0]
    rows_local, width = stream.shape
    experts = sp_size * gate_weight.shape[0]
    top_count = routes.shape[1]
    low = sp < sp_size // 2

    kv = lax.all_gather(jnp.concatenate([key_rows, value_rows], axis=1), "sp", axis=0, tiled=True)
    split = queries.reshape(tp_size, 2, length // (2 * tp_size), queries.shape[1])
    own = split[:, 0].reshape(length // 2, -1)
    other = lax.ppermute(
        split[:, 1].reshape(length // 2, -1), "sp", [(s, sp_size - 1 - s) for s in range(sp_size)]
    )

    mine = (gate_weight[0], up_weight[0], down_weight[0])
    along = moved(sp_size, tp_size, lambda c: 2 * c - 1, 0)
    sibling = moved(sp_size, tp_size, lambda c: 0, 1)
    opposite = moved(sp_size, tp_size, lambda c: tp_size // 4, 0)
    passed = tuple(lax.ppermute(w, BOTH, along) for w in mine)
    mine_too = tuple(lax.ppermute(w, BOTH, sibling) for w in mine)
    passed_too = tuple(lax.ppermute(w, BOTH, sibling) for w in passed)
    sets = (mine, mine_too, passed, passed_too)

    slots = max(2, (rows_local * top_count * 5 + 4 * experts - 1) // (4 * experts))
    part = slots // CHUNKS
    flat = routes.reshape(-1)
    onehot = (flat[:, None] == jnp.arange(experts, dtype=jnp.int32)[None, :]).astype(BF16)
    count = flat.shape[0]
    earlier = (jnp.arange(count)[None, :] < jnp.arange(count)[:, None]).astype(BF16)
    slot = jnp.sum(dot(earlier, onehot) * onehot.astype(F32), axis=1).astype(jnp.int32)
    packed = experts * part * CUTS
    places = jnp.arange(packed, dtype=jnp.int32)

    def hits(k, rows_first):
        e, j = (v.reshape(rows_local, top_count)[:, k] for v in (flat, slot))
        at = jnp.stack(
            [
                jnp.stack([jnp.where(j // part == c, (e * CUTS + n) * part + j % part, -1) for n in range(CUTS)])
                for c in range(CHUNKS)
            ]
        )
        return places[:, None] == at[:, :, None, :] if rows_first else places == at[..., None]

    dispatch = sum(hits(k, True).astype(BF16) for k in range(top_count))
    weighted = sum(jnp.where(hits(k, False), route_weight[:, k : k + 1], 0.0) for k in range(top_count))
    high = weighted.astype(BF16)
    low_part = (weighted - lax.reduce_precision(weighted, 8, 7)).astype(BF16)
    row = jnp.arange(experts * part, dtype=jnp.int32)
    select = jnp.stack(
        [
            (((row // part * CUTS + n) * part + row % part)[:, None] == places).astype(BF16)
            for n in range(CUTS)
        ]
    )

    heads = attention(own, other, kv, lambdas, head_gain, sp, sp_size)
    half = rows_local // 2
    heads = heads.reshape(2 * tp_size, half, 128)
    groups = [
        [s * tp_size + t for s in (n, sp_size - 1 - n) for t in range(tp_size)]
        for n in range(sp_size // 2)
    ]
    heads = lax.all_to_all(
        heads, BOTH, split_axis=0, concat_axis=0, tiled=True, axis_index_groups=groups
    ).reshape(2, tp_size, half, 128)
    heads = jnp.where(low, heads, heads[::-1])

    attended, *outgoing = project(heads, out_weight, stream, ffn_gain, dispatch)

    def exchange(x):
        x = x.reshape(experts, CUTS * part, width // CUTS)
        return lax.all_to_all(x, "sp", split_axis=0, concat_axis=0, tiled=True).reshape(packed, -1)

    arrived = [exchange(x) for x in outgoing]
    theirs = [lax.ppermute(x, BOTH, opposite) for x in arrived]
    kept = [expert(arrived[:1], select, sets, F32)[0]]
    theirs[0], kept[0] = lax.optimization_barrier((theirs[0], kept[0]))
    given = [expert([x], select, sets, BF16)[0] for x in theirs]
    got = [lax.ppermute(x, BOTH, opposite) for x in given]
    filled = [pack(kept[0], got[0], select)]
    last, filled[0] = lax.optimization_barrier((arrived[1], filled[0]))
    kept.append(expert([last], select, sets, F32)[0])
    filled.append(pack(kept[1], got[1], select))
    returned = [exchange(x) for x in filled]
    return combine(returned, high, low_part, attended)


def solution(mesh):
    placed = (
        P("sp", "tp"),
        P("sp", "tp"),
        P("sp", "tp"),
        P("tp"),
        P(),
        P(),
        P(("sp", "tp"), None),
        P(),
        P(("sp", "tp"), None),
        P(("sp", "tp"), None),
        P("sp", None, "tp"),
        P("sp", None, "tp"),
        P("sp", "tp", None),
    )
    return jax.shard_map(
        local, mesh=mesh, in_specs=placed, out_specs=P(("sp", "tp"), None), check_vma=False
    )
```

```python
import math

import jax
import jax.numpy as jnp
from jax import lax
from jax.experimental import pallas as pl
from jax.experimental.pallas import tpu as pltpu
from jax.sharding import PartitionSpec as P

DH = 64
KEYS = 1024
ROWS = 256
SCALE = DH**-0.5 * math.log2(math.e)
BOTH = ("sp", "tp")
F32 = jnp.float32
BF16 = jnp.bfloat16
VMEM_LIMIT = 58 * 1024 * 1024
CHUNKS = 2
CUTS = 4
SHARERS = 2
FLOPS_US = 1.0e9


def dot(a, b, dims=((1,), (0,))):
    return lax.dot_general(a, b, (dims, ((), ())), preferred_element_type=F32)


def attention_body(half_at, key_at, pos_at, out_at, q_ref, k_ref, v_ref, lam_ref, gain_ref, o_ref, m_sc, acc_sc):
    step = pl.program_id(0)
    begin = key_at[step] * KEYS
    q_pos = pos_at[step]
    rows = q_ref.shape[2]

    @pl.when(begin == 0)
    def _():
        m_sc[...] = jnp.full(m_sc.shape, -1e30, F32)
        acc_sc[...] = jnp.zeros(acc_sc.shape, F32)

    last = begin + KEYS > q_pos

    def run(masked):
        k = k_ref[...]
        v = jnp.concatenate([v_ref[...], jnp.ones((KEYS, 128), BF16)], axis=1)
        tiles = [(m, r) for r in range(rows // ROWS) for m in range(2)]

        def scores(m, r):
            s = dot(q_ref[0, m, pl.ds(r * ROWS, ROWS), :], k, ((1,), (1,)))
            if masked:
                row = r * ROWS + lax.broadcasted_iota(jnp.int32, s.shape, 0)
                at = q_pos + lax.shift_right_logical(row, 6) * 128 + (row & 63)
                key = begin + lax.broadcasted_iota(jnp.int32, s.shape, 1)
                s = jnp.where(key <= at, s, -1e30)
            return s

        def finish(m, r, s):
            at = pl.ds(r * ROWS, ROWS)
            old = m_sc[m, at, :]
            new = jnp.maximum(old, jnp.max(s, axis=1, keepdims=True))
            m_sc[m, at, :] = new
            p = jnp.exp2((s - jnp.concatenate([new] * (KEYS // 128), axis=1)) * SCALE)
            factor = jnp.exp2((old - new) * SCALE)
            both = jnp.concatenate([factor, factor], axis=1)
            acc_sc[m, at, :] = acc_sc[m, at, :] * both + dot(p.astype(BF16), v)

        s = scores(*tiles[0])
        for n, tile in enumerate(tiles):
            after = scores(*tiles[n + 1]) if n + 1 < len(tiles) else None
            finish(*tile, s)
            s = after

    @pl.when(jnp.logical_not(last))
    def _():
        run(False)

    @pl.when(last)
    def _():
        run(True)
        first = acc_sc[0, :, :128] / acc_sc[0, :, 128:]
        second = acc_sc[1, :, :128] / acc_sc[1, :, 128:]
        c = first - lam_ref[0] * second
        c = c * lax.rsqrt(jnp.mean(c * c, axis=1, keepdims=True) + 1e-05) * gain_ref[...]
        o_ref[0] = c.astype(BF16)


def attention(own, other, kv, lambdas, gain, sp, sp_size):
    half = own.shape[0]
    zero = jnp.zeros((2, half, DH), BF16)
    q = jnp.stack([other, own])
    q = jnp.stack(
        [
            jnp.concatenate([q[..., :DH], zero], -1),
            jnp.concatenate([zero, q[..., DH:]], -1),
        ],
        1,
    )
    steps = sp_size + 1
    step = jnp.arange(steps, dtype=jnp.int32)
    count = sp_size - sp
    is_other = step < count
    low = sp < sp_size // 2
    half_at = jnp.where(is_other, 0, 1).astype(jnp.int32)
    key_at = jnp.where(is_other, step, step - count).astype(jnp.int32)
    pos_at = jnp.where(is_other, (sp_size - 1 - sp) * KEYS + 64, sp * KEYS).astype(jnp.int32)
    out_at = jnp.where(is_other == low, 1, 0).astype(jnp.int32)
    spec = pltpu.PrefetchScalarGridSpec(
        num_scalar_prefetch=4,
        grid=(steps,),
        in_specs=[
            pl.BlockSpec((1, 2, half, 128), lambda s, h, k, p, o: (h[s], 0, 0, 0)),
            pl.BlockSpec((KEYS, 128), lambda s, h, k, p, o: (k[s], 0)),
            pl.BlockSpec((KEYS, 128), lambda s, h, k, p, o: (k[s], 1)),
            pl.BlockSpec(memory_space=pltpu.SMEM),
            pl.BlockSpec((1, 128), lambda s, h, k, p, o: (0, 0)),
        ],
        out_specs=pl.BlockSpec((1, half, 128), lambda s, h, k, p, o: (o[s], 0, 0)),
        scratch_shapes=[pltpu.VMEM((2, half, 128), F32), pltpu.VMEM((2, half, 256), F32)],
    )
    return pl.pallas_call(
        attention_body,
        grid_spec=spec,
        out_shape=jax.ShapeDtypeStruct((2, half, 128), BF16),
        compiler_params=pltpu.CompilerParams(
            dimension_semantics=("arbitrary",), vmem_limit_bytes=VMEM_LIMIT
        ),
        cost_estimate=cost(29),
        name="attention",
    )(half_at, key_at, pos_at, out_at, q, kv, kv, lambdas, gain.reshape(1, 128))


def project_body(h_ref, w_ref, s_ref, g_ref, d_ref, a_ref, *o_refs):
    parts = [jnp.concatenate([h_ref[n, t] for t in range(h_ref.shape[1])], axis=1) for n in range(2)]
    x = jnp.concatenate(parts, axis=0)
    attended = s_ref[...].astype(F32) + dot(x, w_ref[...])
    a_ref[...] = attended
    mean = jnp.mean(attended * attended, axis=1, keepdims=True)
    normed = (attended * lax.rsqrt(mean + 1e-06) * g_ref[...]).astype(BF16)
    for c, o_ref in enumerate(o_refs):
        rows = sum(dot(d_ref[c, n], cut(normed, n)) for n in range(CUTS)).astype(BF16)
        for h in range(SHARERS):
            o_ref[h] = rows


def cut(x, n):
    wide = x.shape[1] // CUTS
    return x[:, n * wide : (n + 1) * wide]


def project(heads, out_weight, stream, gain, dispatch):
    rows, width = stream.shape
    packed = jax.ShapeDtypeStruct((SHARERS, dispatch.shape[2], width // CUTS), BF16)
    return pl.pallas_call(
        project_body,
        out_shape=(jax.ShapeDtypeStruct((rows, width), F32),) + (packed,) * CHUNKS,
        compiler_params=pltpu.CompilerParams(vmem_limit_bytes=VMEM_LIMIT),
        cost_estimate=cost(5),
        name="project",
    )(heads, out_weight, stream, gain.reshape(1, width), dispatch)


def cost(microseconds):
    return pl.CostEstimate(flops=int(microseconds * FLOPS_US), bytes_accessed=0, transcendentals=0)


def expert_body(sets, r_any, s_any, *refs):
    weights = refs[: 3 * sets]
    o_ref, r_ref, s_ref, x_sc, acc_sc, in_buf, down_buf, sem, small = refs[3 * sets :]
    hidden = in_buf.shape[2] // 2
    rows = s_ref.shape[1]

    def copy(n, kind):
        if kind < 2:
            to = in_buf.at[n, :, pl.ds(kind * hidden, hidden)]
        else:
            to = down_buf.at[n // 2, pl.ds(n % 2 * hidden, hidden), :]
        return pltpu.make_async_copy(weights[3 * n + kind], to, sem.at[3 * n + kind])

    first = pltpu.make_async_copy(r_any, r_ref, small.at[0])
    second = pltpu.make_async_copy(s_any, s_ref, small.at[1])
    first.start()
    second.start()
    for p in range(sets // 2):
        for n, kind in ((0, 0), (0, 1), (1, 0), (1, 1), (0, 2), (1, 2)):
            copy(2 * p + n, kind).start()
    first.wait()
    second.wait()
    wide = r_ref.shape[2]
    for h in range(SHARERS):
        for n in range(CUTS):
            x_sc[h * rows : (h + 1) * rows, n * wide : (n + 1) * wide] = dot(s_ref[n], r_ref[h]).astype(BF16)
    x = x_sc[...]
    for p in range(sets // 2):
        acts = []
        for n in (2 * p, 2 * p + 1):
            copy(n, 0).wait()
            copy(n, 1).wait()
            both = dot(x, in_buf[n])
            gate, upper = both[:, :hidden], both[:, hidden:]
            acts.append((gate / (1.0 + jnp.exp(-gate)) * upper).astype(BF16))
        copy(2 * p, 2).wait()
        copy(2 * p + 1, 2).wait()
        part = dot(jnp.concatenate(acts, axis=1), down_buf[p])
        if p == 0:
            acc_sc[...] = part
        elif p + 1 < sets // 2:
            acc_sc[...] += part
        else:
            whole = (acc_sc[...] + part).astype(BF16)
            for h in range(SHARERS):
                mine = whole[h * rows : (h + 1) * rows]
                o_ref[h] = sum(
                    dot(s_ref[n], cut(mine, n), ((0,), (0,))) for n in range(CUTS)
                ).astype(BF16)


def expert(arrived, select, sets):
    rows = SHARERS * select.shape[1]
    width, hidden = sets[0][0].shape
    flat = [w for one in sets for w in one]
    return pl.pallas_call(
        lambda *refs: expert_body(len(sets), *refs),
        in_specs=[pl.BlockSpec(memory_space=pl.ANY)] * (2 + len(flat)),
        out_specs=pl.BlockSpec(memory_space=pltpu.VMEM),
        out_shape=jax.ShapeDtypeStruct(arrived.shape, BF16),
        scratch_shapes=[
            pltpu.VMEM(arrived.shape, BF16),
            pltpu.VMEM(select.shape, BF16),
            pltpu.VMEM((rows, width), BF16),
            pltpu.VMEM((rows, width), F32),
            pltpu.VMEM((len(sets), width, 2 * hidden), BF16),
            pltpu.VMEM((len(sets) // 2, 2 * hidden, width), BF16),
            pltpu.SemaphoreType.DMA((len(flat),)),
            pltpu.SemaphoreType.DMA((2,)),
        ],
        compiler_params=pltpu.CompilerParams(vmem_limit_bytes=VMEM_LIMIT),
        cost_estimate=cost(16),
        name="expert",
    )(arrived, select, *flat)


def combine_body(*refs):
    r_refs, (high_ref, low_ref, a_ref, o_ref) = refs[:CHUNKS], refs[CHUNKS:]
    wide = r_refs[0].shape[2]
    rows = [sum(r_ref[h].astype(F32) for h in range(SHARERS)).astype(BF16) for r_ref in r_refs]
    for n in range(CUTS):
        at = slice(n * wide, n * wide + wide)
        routed = a_ref[:, at]
        for c, r in enumerate(rows):
            routed = routed + dot(high_ref[c, n], r) + dot(low_ref[c, n], r)
        o_ref[:, at] = routed.astype(BF16)


def combine(returned, high, low, attended):
    return pl.pallas_call(
        combine_body,
        out_shape=jax.ShapeDtypeStruct(attended.shape, BF16),
        compiler_params=pltpu.CompilerParams(vmem_limit_bytes=VMEM_LIMIT),
        name="combine",
    )(*returned, high, low, attended)


def moved(sp_size, tp_size, shift, flip):
    pairs = []
    for s in range(sp_size):
        for t in range(tp_size):
            y, c = t // 2, t % 2
            to = (y + shift(c)) % (tp_size // 2) * 2 + (c ^ flip)
            pairs.append((s * tp_size + t, s * tp_size + to))
    return pairs


def local(
    queries,
    key_rows,
    value_rows,
    lambdas,
    head_gain,
    out_weight,
    stream,
    ffn_gain,
    routes,
    route_weight,
    gate_weight,
    up_weight,
    down_weight,
):
    sp_size = lax.axis_size("sp")
    tp_size = lax.axis_size("tp")
    sp = lax.axis_index("sp")
    length = queries.shape[0]
    rows_local, width = stream.shape
    experts = sp_size * gate_weight.shape[0]
    top_count = routes.shape[1]
    low = sp < sp_size // 2

    kv = lax.all_gather(jnp.concatenate([key_rows, value_rows], axis=1), "sp", axis=0, tiled=True)
    split = queries.reshape(tp_size, 2, length // (2 * tp_size), queries.shape[1])
    own = split[:, 0].reshape(length // 2, -1)
    other = lax.ppermute(
        split[:, 1].reshape(length // 2, -1), "sp", [(s, sp_size - 1 - s) for s in range(sp_size)]
    )

    mine = (gate_weight[0], up_weight[0], down_weight[0])
    along = moved(sp_size, tp_size, lambda c: 2 * c - 1, 0)
    sibling = moved(sp_size, tp_size, lambda c: 0, 1)
    passed = tuple(lax.ppermute(w, BOTH, along) for w in mine)
    mine_too = tuple(lax.ppermute(w, BOTH, sibling) for w in mine)

    slots = max(2, (rows_local * top_count * 5 + 4 * experts - 1) // (4 * experts))
    part = slots // CHUNKS
    flat = routes.reshape(-1)
    onehot = (flat[:, None] == jnp.arange(experts, dtype=jnp.int32)[None, :]).astype(BF16)
    count = flat.shape[0]
    earlier = (jnp.arange(count)[None, :] < jnp.arange(count)[:, None]).astype(BF16)
    slot = jnp.sum(dot(earlier, onehot) * onehot.astype(F32), axis=1).astype(jnp.int32)
    packed = experts * part * CUTS
    places = jnp.arange(packed, dtype=jnp.int32)

    def hits(k, rows_first):
        e, j = (v.reshape(rows_local, top_count)[:, k] for v in (flat, slot))
        at = jnp.stack(
            [
                jnp.stack([jnp.where(j // part == c, (e * CUTS + n) * part + j % part, -1) for n in range(CUTS)])
                for c in range(CHUNKS)
            ]
        )
        return places[:, None] == at[:, :, None, :] if rows_first else places == at[..., None]

    dispatch = sum(hits(k, True).astype(BF16) for k in range(top_count))
    weighted = sum(jnp.where(hits(k, False), route_weight[:, k : k + 1], 0.0) for k in range(top_count))
    high = weighted.astype(BF16)
    low_part = (weighted - lax.reduce_precision(weighted, 8, 7)).astype(BF16)
    row = jnp.arange(experts * part, dtype=jnp.int32)
    select = jnp.stack(
        [
            (((row // part * CUTS + n) * part + row % part)[:, None] == places).astype(BF16)
            for n in range(CUTS)
        ]
    )

    heads = attention(own, other, kv, lambdas, head_gain, sp, sp_size)
    half = rows_local // 2
    heads = heads.reshape(2 * tp_size, half, 128)
    groups = [
        [s * tp_size + t for s in (n, sp_size - 1 - n) for t in range(tp_size)]
        for n in range(sp_size // 2)
    ]
    heads = lax.all_to_all(
        heads, BOTH, split_axis=0, concat_axis=0, tiled=True, axis_index_groups=groups
    ).reshape(2, tp_size, half, 128)
    heads = jnp.where(low, heads, heads[::-1])

    attended, *outgoing = project(heads, out_weight, stream, ffn_gain, dispatch)

    passed, outgoing = lax.optimization_barrier((passed, outgoing))
    passed_too = tuple(lax.ppermute(w, BOTH, sibling) for w in passed)
    sets = (mine, mine_too, passed, passed_too)

    ring = tp_size // 2
    members = [
        [
            s * tp_size + (y + h * (ring // SHARERS)) * 2 + c
            for h in range(SHARERS)
            for s in range(sp_size)
        ]
        for y in range(ring // SHARERS)
        for c in range(2)
    ]

    def exchange(x):
        x = x.reshape(SHARERS * experts, CUTS * part, width // CUTS)
        return lax.all_to_all(
            x, BOTH, split_axis=0, concat_axis=0, tiled=True, axis_index_groups=members
        ).reshape(SHARERS, packed, width // CUTS)

    arrived = [exchange(x) for x in outgoing]
    returned = [exchange(expert(x, select, sets)) for x in arrived]
    return combine(returned, high, low_part, attended)


def solution(mesh):
    placed = (
        P("sp", "tp"),
        P("sp", "tp"),
        P("sp", "tp"),
        P("tp"),
        P(),
        P(),
        P(("sp", "tp"), None),
        P(),
        P(("sp", "tp"), None),
        P(("sp", "tp"), None),
        P("sp", None, "tp"),
        P("sp", None, "tp"),
        P("sp", "tp", None),
    )
    return jax.shard_map(
        local, mesh=mesh, in_specs=placed, out_specs=P(("sp", "tp"), None), check_vma=False
    )
```

```python
import math

import jax
import jax.numpy as jnp
from jax import lax
from jax.experimental import pallas as pl
from jax.experimental.pallas import tpu as pltpu
from jax.sharding import PartitionSpec as P

DH = 64
PIECE = 512
ROWS = 256
SCALE = DH**-0.5 * math.log2(math.e)
BOTH = ("sp", "tp")
F32 = jnp.float32
BF16 = jnp.bfloat16
VMEM_LIMIT = 58 * 1024 * 1024
CHUNKS = 2
CUTS = 4
SHARERS = 2
FLOPS_US = 1.0e9


def dot(a, b, dims=((1,), (0,))):
    return lax.dot_general(a, b, (dims, ((), ())), preferred_element_type=F32)


def attention_body(pieces, side, first, final, count, *refs):
    sp_ref, lam_ref, gain_ref, q_ref = refs[:4]
    kv_refs, refs = refs[4 : 4 + count], refs[4 + count :]
    if first:
        m_ref, acc_ref = None, None
    else:
        (m_ref, acc_ref), refs = refs[:2], refs[2:]
    if final:
        (o_ref, m_sc, acc_sc), refs = refs[:3], refs[3:]
    else:
        (m_sc, acc_sc), refs = refs[:2], refs[2:]
    kv, sem, order, base_at, bounds = refs[:5]
    sp = sp_ref[0]
    z, x = sp // side, sp % side
    blocks = side * side
    begin = 0
    copies = []
    for n, ref in enumerate(kv_refs):
        copies.append(pltpu.make_async_copy(ref, kv.at[pl.ds(begin, ref.shape[0])], sem.at[n]))
        begin += ref.shape[0]
    for c in copies:
        c.start()
    if first:
        m_sc[...] = jnp.full(m_sc.shape, -1e30, F32)
        acc_sc[...] = jnp.zeros(acc_sc.shape, F32)
    else:
        m_sc[...] = m_ref[...]
        acc_sc[...] = acc_ref[...]

    mine = (blocks - 1 - sp, sp)
    for n, (dz, dx, low) in enumerate(pieces):
        block = (z + dz + side) % side * side + (x + dx + side) % side
        base_at[n] = block * (2 * PIECE) + low * PIECE
        for h in range(2):
            spot = jnp.int32(0) if n == 0 else bounds[h]
            order[h, spot] = jnp.int32(n)
            bounds[h] = spot + (block < mine[h]).astype(jnp.int32)
    for h in range(2):
        spot = bounds[h]
        for n in range(len(pieces)):
            order[h, spot] = jnp.int32(n)
            spot = spot + (base_at[n] // (2 * PIECE) == mine[h]).astype(jnp.int32)
        bounds[2 + h] = spot
    for c in copies:
        c.wait()

    rows = q_ref.shape[2]

    def step(h, at, masked):
        parts = [kv[pl.ds(pl.multiple_of(p * PIECE, PIECE), PIECE), :] for p in at]
        keys = len(at) * PIECE
        k = jnp.concatenate([p[:, :128] for p in parts], axis=0)
        v = jnp.concatenate([p[:, 128:] for p in parts], axis=0)
        v = jnp.concatenate([v, jnp.ones((keys, 128), BF16)], axis=1)
        tiles = [(m, r) for r in range(rows // ROWS) for m in range(2)]

        def scores(m, r):
            s = dot(q_ref[h, m, pl.ds(r * ROWS, ROWS), :], k, ((1,), (1,)))
            if masked:
                row = r * ROWS + lax.broadcasted_iota(jnp.int32, s.shape, 0)
                start = jnp.where(h == 0, (blocks - 1 - sp) * (2 * PIECE) + 64, sp * (2 * PIECE))
                q_at = start + lax.shift_right_logical(row, 6) * 128 + (row & 63)
                key = lax.broadcasted_iota(jnp.int32, s.shape, 1)
                key = key + jnp.where(key < PIECE, base_at[at[0]], base_at[at[-1]] - (keys - PIECE))
                s = jnp.where(key <= q_at, s, -1e30)
            return s

        def finish(m, r, s):
            to = pl.ds(r * ROWS, ROWS)
            old = m_sc[h, m, to, :]
            new = jnp.maximum(old, jnp.max(s, axis=1, keepdims=True))
            m_sc[h, m, to, :] = new
            p = jnp.exp2((s - jnp.concatenate([new] * (keys // 128), axis=1)) * SCALE)
            factor = jnp.exp2((old - new) * SCALE)
            both = jnp.concatenate([factor, factor], axis=1)
            acc_sc[h, m, to, :] = acc_sc[h, m, to, :] * both + dot(p.astype(BF16), v)

        s = scores(*tiles[0])
        for n, tile in enumerate(tiles):
            after = scores(*tiles[n + 1]) if n + 1 < len(tiles) else None
            finish(*tile, s)
            s = after

    def half(h, carry):
        number = bounds[h]

        def pair(n, inner):
            step(h, (order[h, 2 * n], order[h, 2 * n + 1]), False)
            return inner

        lax.fori_loop(0, number // 2, pair, 0)

        @pl.when(number % 2 == 1)
        def _():
            step(h, (order[h, number - 1],), False)

        if not final:

            @pl.when(bounds[2 + h] > number)
            def _():
                step(h, (order[h, number], order[h, number + 1]), True)

        return carry

    lax.fori_loop(0, 2, half, 0)
    if final:
        for h in range(2):
            c0 = acc_sc[h, 0, :, :128] / acc_sc[h, 0, :, 128:]
            c1 = acc_sc[h, 1, :, :128] / acc_sc[h, 1, :, 128:]
            c = c0 - lam_ref[0] * c1
            c = c * lax.rsqrt(jnp.mean(c * c, axis=1, keepdims=True) + 1e-05) * gain_ref[...]
            o_ref[jnp.where(sp < blocks // 2, 1 - h, h)] = c.astype(BF16)


def attention(q, arrays, pieces, state, lambdas, gain, sp, side, final):
    half = q.shape[2]
    first = state is None
    whole = pl.BlockSpec(memory_space=pltpu.VMEM)
    scalar = pl.BlockSpec(memory_space=pltpu.SMEM)
    held = (
        jax.ShapeDtypeStruct((2, 2, half, 128), F32),
        jax.ShapeDtypeStruct((2, 2, half, 256), F32),
    )
    scratch = [
        pltpu.VMEM((len(pieces) * PIECE, arrays[0].shape[1]), BF16),
        pltpu.SemaphoreType.DMA((len(arrays),)),
        pltpu.SMEM((2, len(pieces) + 2), jnp.int32),
        pltpu.SMEM((len(pieces),), jnp.int32),
        pltpu.SMEM((4,), jnp.int32),
    ]
    if final:
        scratch = [pltpu.VMEM(h.shape, F32) for h in held] + scratch
    return pl.pallas_call(
        lambda *refs: attention_body(pieces, side, first, final, len(arrays), *refs),
        in_specs=[scalar, scalar, whole, whole]
        + [pl.BlockSpec(memory_space=pl.ANY)] * len(arrays)
        + ([] if first else [whole, whole]),
        out_specs=whole if final else (whole, whole),
        out_shape=jax.ShapeDtypeStruct((2, half, 128), BF16) if final else held,
        scratch_shapes=scratch,
        compiler_params=pltpu.CompilerParams(vmem_limit_bytes=VMEM_LIMIT),
        cost_estimate=cost(len(pieces)),
        name="attention",
    )(sp.reshape(1), lambdas, gain.reshape(1, 128), q, *arrays, *(() if first else state))


def spread(array, forth, back):
    half = array.shape[0] // 2
    before, behind = lax.ppermute(array, "sp", forth), lax.ppermute(array, "sp", back)
    far = lax.ppermute(before[:half], "sp", forth), lax.ppermute(behind[half:], "sp", back)
    return (before, behind), far


def attend(queries, key_rows, value_rows, lambdas, head_gain):
    sp_size, tp_size = lax.axis_size("sp"), lax.axis_size("tp")
    side = math.isqrt(sp_size)
    sp = lax.axis_index("sp")
    length = queries.shape[0]
    kv = jnp.concatenate([key_rows, value_rows], axis=1)
    ring = {}
    for name, dz, dx in (("z+", 1, 0), ("z-", -1, 0), ("x+", 0, 1), ("x-", 0, -1)):
        ring[name] = [
            (s, (s // side + dz) % side * side + (s % side + dx) % side) for s in range(sp_size)
        ]
    along_z, along_x = (ring["z+"], ring["z-"]), (ring["x+"], ring["x-"])
    upper, lower = kv[: length // 2], kv[length // 2 :]
    split = queries.reshape(tp_size, 2, length // (2 * tp_size), queries.shape[1])
    own = split[:, 0].reshape(length // 2, -1)
    near_u, far_u = spread(upper, *along_x)
    near_l, far_l = spread(lower, *along_z)
    other = lax.ppermute(
        split[:, 1].reshape(length // 2, -1), "sp", [(s, sp_size - 1 - s) for s in range(sp_size)]
    )
    row = jnp.concatenate([upper, *near_u, *far_u], axis=0)
    column = jnp.concatenate([lower, *near_l, *far_l], axis=0)
    near_row, far_row = spread(row, *along_z)
    near_column, far_column = spread(column, *along_x)
    steps = (0, -1, 1, 2)

    zero = jnp.zeros((2, length // 2, DH), BF16)
    q = jnp.stack([other, own])
    q = jnp.stack(
        [jnp.concatenate([q[..., :DH], zero], -1), jnp.concatenate([zero, q[..., DH:]], -1)], 1
    )
    calls = (
        ((row, column), [(0, d, 0) for d in steps] + [(d, 0, 1) for d in steps]),
        (
            near_row + near_column,
            [(e, d, 0) for e in (-1, 1) for d in steps] + [(d, e, 1) for e in (-1, 1) for d in steps],
        ),
        (far_row + far_column, [(2, d, 0) for d in steps] + [(d, 2, 1) for d in steps]),
    )
    state = None
    for n, (arrays, pieces) in enumerate(calls):
        state = attention(
            q, arrays, pieces, state, lambdas, head_gain, sp, side, n + 1 == len(calls)
        )
    return state


def project_body(h_ref, w_ref, s_ref, g_ref, d_ref, a_ref, *o_refs):
    parts = [jnp.concatenate([h_ref[n, t] for t in range(h_ref.shape[1])], axis=1) for n in range(2)]
    x = jnp.concatenate(parts, axis=0)
    attended = s_ref[...].astype(F32) + dot(x, w_ref[...])
    a_ref[...] = attended
    mean = jnp.mean(attended * attended, axis=1, keepdims=True)
    normed = (attended * lax.rsqrt(mean + 1e-06) * g_ref[...]).astype(BF16)
    for c, o_ref in enumerate(o_refs):
        rows = sum(dot(d_ref[c, n], cut(normed, n)) for n in range(CUTS)).astype(BF16)
        for h in range(SHARERS):
            o_ref[h] = rows


def cut(x, n):
    wide = x.shape[1] // CUTS
    return x[:, n * wide : (n + 1) * wide]


def project(heads, out_weight, stream, gain, dispatch):
    rows, width = stream.shape
    packed = jax.ShapeDtypeStruct((SHARERS, dispatch.shape[2], width // CUTS), BF16)
    return pl.pallas_call(
        project_body,
        out_shape=(jax.ShapeDtypeStruct((rows, width), F32),) + (packed,) * CHUNKS,
        compiler_params=pltpu.CompilerParams(vmem_limit_bytes=VMEM_LIMIT),
        cost_estimate=cost(5),
        name="project",
    )(heads, out_weight, stream, gain.reshape(1, width), dispatch)


def cost(microseconds):
    return pl.CostEstimate(flops=int(microseconds * FLOPS_US), bytes_accessed=0, transcendentals=0)


def expert_body(sets, r_any, s_any, p_any, *refs):
    weights = refs[: 3 * sets]
    o_ref, r_ref, s_ref, p_ref, x_sc, acc_sc, in_buf, down_buf, sem, small = refs[3 * sets :]
    hidden = in_buf.shape[2] // 2
    rows = s_ref.shape[1]

    def copy(n, kind):
        if kind < 2:
            to = in_buf.at[n, :, pl.ds(kind * hidden, hidden)]
        else:
            to = down_buf.at[n // 2, pl.ds(n % 2 * hidden, hidden), :]
        return pltpu.make_async_copy(weights[3 * n + kind], to, sem.at[3 * n + kind])

    first = pltpu.make_async_copy(r_any, r_ref, small.at[0])
    second = pltpu.make_async_copy(s_any, s_ref, small.at[1])
    third = pltpu.make_async_copy(p_any, p_ref, small.at[2])
    first.start()
    second.start()
    for p in range(sets // 2):
        for n, kind in ((0, 0), (0, 1), (1, 0), (1, 1), (0, 2), (1, 2)):
            copy(2 * p + n, kind).start()
    third.start()
    first.wait()
    second.wait()
    wide = r_ref.shape[2]
    for h in range(SHARERS):
        for n in range(CUTS):
            x_sc[h * rows : (h + 1) * rows, n * wide : (n + 1) * wide] = dot(s_ref[n], r_ref[h]).astype(BF16)
    x = x_sc[...]
    third.wait()
    for p in range(sets // 2):
        acts = []
        for n in (2 * p, 2 * p + 1):
            copy(n, 0).wait()
            copy(n, 1).wait()
            both = dot(x, in_buf[n])
            gate, upper = both[:, :hidden], both[:, hidden:]
            acts.append((gate / (1.0 + jnp.exp(-gate)) * upper).astype(BF16))
        copy(2 * p, 2).wait()
        copy(2 * p + 1, 2).wait()
        part = dot(jnp.concatenate(acts, axis=1), down_buf[p])
        if p == 0:
            acc_sc[...] = part
        elif p + 1 < sets // 2:
            acc_sc[...] += part
        else:
            whole = (acc_sc[...] + part).astype(BF16)
            for h in range(SHARERS):
                mine = whole[h * rows : (h + 1) * rows]
                o_ref[h] = sum(dot(p_ref[n], cut(mine, n)) for n in range(CUTS)).astype(BF16)


def expert(arrived, select, place, sets):
    rows = SHARERS * select.shape[1]
    width, hidden = sets[0][0].shape
    flat = [w for one in sets for w in one]
    return pl.pallas_call(
        lambda *refs: expert_body(len(sets), *refs),
        in_specs=[pl.BlockSpec(memory_space=pl.ANY)] * (3 + len(flat)),
        out_specs=pl.BlockSpec(memory_space=pltpu.VMEM),
        out_shape=jax.ShapeDtypeStruct(arrived.shape, BF16),
        scratch_shapes=[
            pltpu.VMEM(arrived.shape, BF16),
            pltpu.VMEM(select.shape, BF16),
            pltpu.VMEM(place.shape, BF16),
            pltpu.VMEM((rows, width), BF16),
            pltpu.VMEM((rows, width), F32),
            pltpu.VMEM((len(sets), width, 2 * hidden), BF16),
            pltpu.VMEM((len(sets) // 2, 2 * hidden, width), BF16),
            pltpu.SemaphoreType.DMA((len(flat),)),
            pltpu.SemaphoreType.DMA((3,)),
        ],
        compiler_params=pltpu.CompilerParams(vmem_limit_bytes=VMEM_LIMIT),
        cost_estimate=cost(16),
        name="expert",
    )(arrived, select, place, *flat)


def combine_body(*refs):
    r_refs, (high_ref, low_ref, a_ref, o_ref) = refs[:CHUNKS], refs[CHUNKS:]
    wide = r_refs[0].shape[2]
    rows = [sum(r_ref[h].astype(F32) for h in range(SHARERS)).astype(BF16) for r_ref in r_refs]
    for n in range(CUTS):
        at = slice(n * wide, n * wide + wide)
        routed = a_ref[:, at]
        for c, r in enumerate(rows):
            routed = routed + dot(high_ref[c, n], r) + dot(low_ref[c, n], r)
        o_ref[:, at] = routed.astype(BF16)


def combine(returned, high, low, attended):
    return pl.pallas_call(
        combine_body,
        out_shape=jax.ShapeDtypeStruct(attended.shape, BF16),
        compiler_params=pltpu.CompilerParams(vmem_limit_bytes=VMEM_LIMIT),
        name="combine",
    )(*returned, high, low, attended)


def moved(sp_size, tp_size, shift, flip):
    pairs = []
    for s in range(sp_size):
        for t in range(tp_size):
            y, c = t // 2, t % 2
            to = (y + shift(c)) % (tp_size // 2) * 2 + (c ^ flip)
            pairs.append((s * tp_size + t, s * tp_size + to))
    return pairs


def local(
    queries,
    key_rows,
    value_rows,
    lambdas,
    head_gain,
    out_weight,
    stream,
    ffn_gain,
    routes,
    route_weight,
    gate_weight,
    up_weight,
    down_weight,
):
    sp_size = lax.axis_size("sp")
    tp_size = lax.axis_size("tp")
    sp = lax.axis_index("sp")
    rows_local, width = stream.shape
    experts = sp_size * gate_weight.shape[0]
    top_count = routes.shape[1]
    low = sp < sp_size // 2

    mine = (gate_weight[0], up_weight[0], down_weight[0])
    along = moved(sp_size, tp_size, lambda c: 2 * c - 1, 0)
    sibling = moved(sp_size, tp_size, lambda c: 0, 1)
    passed = tuple(lax.ppermute(w, BOTH, along) for w in mine)
    mine_too = tuple(lax.ppermute(w, BOTH, sibling) for w in mine)

    slots = max(2, (rows_local * top_count * 5 + 4 * experts - 1) // (4 * experts))
    part = slots // CHUNKS
    flat = routes.reshape(-1)
    onehot = (flat[:, None] == jnp.arange(experts, dtype=jnp.int32)[None, :]).astype(BF16)
    count = flat.shape[0]
    earlier = (jnp.arange(count)[None, :] < jnp.arange(count)[:, None]).astype(BF16)
    slot = jnp.sum(dot(earlier, onehot) * onehot.astype(F32), axis=1).astype(jnp.int32)
    packed = experts * part * CUTS
    places = jnp.arange(packed, dtype=jnp.int32)

    def hits(k, rows_first):
        e, j = (v.reshape(rows_local, top_count)[:, k] for v in (flat, slot))
        at = jnp.stack(
            [
                jnp.stack([jnp.where(j // part == c, (e * CUTS + n) * part + j % part, -1) for n in range(CUTS)])
                for c in range(CHUNKS)
            ]
        )
        return places[:, None] == at[:, :, None, :] if rows_first else places == at[..., None]

    dispatch = sum(hits(k, True).astype(BF16) for k in range(top_count))
    weighted = sum(jnp.where(hits(k, False), route_weight[:, k : k + 1], 0.0) for k in range(top_count))
    high = weighted.astype(BF16)
    low_part = (weighted - lax.reduce_precision(weighted, 8, 7)).astype(BF16)
    row = jnp.arange(experts * part, dtype=jnp.int32)
    cuts = jnp.stack([(row // part * CUTS + n) * part + row % part for n in range(CUTS)])
    select = (cuts[:, :, None] == places).astype(BF16)
    place = (places[:, None] == cuts[:, None, :]).astype(BF16)

    heads = attend(queries, key_rows, value_rows, lambdas, head_gain)
    half = rows_local // 2
    heads = heads.reshape(2 * tp_size, half, 128)
    groups = [
        [s * tp_size + t for s in (n, sp_size - 1 - n) for t in range(tp_size)]
        for n in range(sp_size // 2)
    ]
    heads = lax.all_to_all(
        heads, BOTH, split_axis=0, concat_axis=0, tiled=True, axis_index_groups=groups
    ).reshape(2, tp_size, half, 128)
    heads = jnp.where(low, heads, heads[::-1])

    attended, *outgoing = project(heads, out_weight, stream, ffn_gain, dispatch)

    passed, outgoing = lax.optimization_barrier((passed, outgoing))
    passed_too = tuple(lax.ppermute(w, BOTH, sibling) for w in passed)
    sets = (mine, mine_too, passed, passed_too)

    ring = tp_size // 2
    members = [
        [
            s * tp_size + (y + h * (ring // SHARERS)) * 2 + c
            for h in range(SHARERS)
            for s in range(sp_size)
        ]
        for y in range(ring // SHARERS)
        for c in range(2)
    ]

    def exchange(x):
        x = x.reshape(SHARERS * experts, CUTS * part, width // CUTS)
        return lax.all_to_all(
            x, BOTH, split_axis=0, concat_axis=0, tiled=True, axis_index_groups=members
        ).reshape(SHARERS, packed, width // CUTS)

    arrived = [exchange(x) for x in outgoing]
    returned = [exchange(expert(x, select, place, sets)) for x in arrived]
    return combine(returned, high, low_part, attended)


def solution(mesh):
    placed = (
        P("sp", "tp"),
        P("sp", "tp"),
        P("sp", "tp"),
        P("tp"),
        P(),
        P(),
        P(("sp", "tp"), None),
        P(),
        P(("sp", "tp"), None),
        P(("sp", "tp"), None),
        P("sp", None, "tp"),
        P("sp", None, "tp"),
        P("sp", "tp", None),
    )
    return jax.shard_map(
        local, mesh=mesh, in_specs=placed, out_specs=P(("sp", "tp"), None), check_vma=False
    )
```

```python
import math

import jax
import jax.numpy as jnp
from jax import lax
from jax.experimental import pallas as pl
from jax.experimental.pallas import tpu as pltpu
from jax.sharding import PartitionSpec as P

DH = 64
PIECE = 512
ROWS = 256
SCALE = DH**-0.5 * math.log2(math.e)
BOTH = ("sp", "tp")
F32 = jnp.float32
BF16 = jnp.bfloat16
VMEM_LIMIT = 58 * 1024 * 1024
ATTENTION_LIMIT = 26 * 1024 * 1024
CHUNKS = 2
CUTS = 4
SHARERS = 2
FLOPS_US = 1.0e9


def dot(a, b, dims=((1,), (0,))):
    return lax.dot_general(a, b, (dims, ((), ())), preferred_element_type=F32)


def attention_body(pieces, side, first, final, count, *refs):
    sp_ref, lam_ref, gain_ref, q_ref = refs[:4]
    kv_refs, refs = refs[4 : 4 + count], refs[4 + count :]
    if first:
        m_ref, acc_ref = None, None
    else:
        (m_ref, acc_ref), refs = refs[:2], refs[2:]
    if final:
        (o_ref, m_sc, acc_sc), refs = refs[:3], refs[3:]
    else:
        (m_sc, acc_sc), refs = refs[:2], refs[2:]
    kv, sem, order, base_at, bounds = refs[:5]
    sp = sp_ref[0]
    z, x = sp // side, sp % side
    blocks = side * side
    begin = 0
    copies = []
    for n, ref in enumerate(kv_refs):
        copies.append(pltpu.make_async_copy(ref, kv.at[pl.ds(begin, ref.shape[0])], sem.at[n]))
        begin += ref.shape[0]
    for c in copies:
        c.start()
    if first:
        m_sc[...] = jnp.full(m_sc.shape, -1e30, F32)
        acc_sc[...] = jnp.zeros(acc_sc.shape, F32)
    else:
        m_sc[...] = m_ref[...]
        acc_sc[...] = acc_ref[...]

    mine = (blocks - 1 - sp, sp)
    for n, (dz, dx, low) in enumerate(pieces):
        block = (z + dz + side) % side * side + (x + dx + side) % side
        base_at[n] = block * (2 * PIECE) + low * PIECE
        for h in range(2):
            spot = jnp.int32(0) if n == 0 else bounds[h]
            order[h, spot] = jnp.int32(n)
            bounds[h] = spot + (block < mine[h]).astype(jnp.int32)
    for h in range(2):
        spot = bounds[h]
        for n in range(len(pieces)):
            order[h, spot] = jnp.int32(n)
            spot = spot + (base_at[n] // (2 * PIECE) == mine[h]).astype(jnp.int32)
        bounds[2 + h] = spot
    for c in copies:
        c.wait()

    rows = q_ref.shape[2]

    def step(h, at, masked):
        parts = [kv[pl.ds(pl.multiple_of(p * PIECE, PIECE), PIECE), :] for p in at]
        keys = len(at) * PIECE
        k = jnp.concatenate([p[:, :128] for p in parts], axis=0)
        v = jnp.concatenate([p[:, 128:] for p in parts], axis=0)
        v = jnp.concatenate([v, jnp.ones((keys, 128), BF16)], axis=1)
        tiles = [(m, r) for r in range(rows // ROWS) for m in range(2)]

        def scores(m, r):
            s = dot(q_ref[h, m, pl.ds(r * ROWS, ROWS), :], k, ((1,), (1,)))
            if masked:
                row = r * ROWS + lax.broadcasted_iota(jnp.int32, s.shape, 0)
                start = jnp.where(h == 0, (blocks - 1 - sp) * (2 * PIECE) + 64, sp * (2 * PIECE))
                q_at = start + lax.shift_right_logical(row, 6) * 128 + (row & 63)
                key = lax.broadcasted_iota(jnp.int32, s.shape, 1)
                key = key + jnp.where(key < PIECE, base_at[at[0]], base_at[at[-1]] - (keys - PIECE))
                s = jnp.where(key <= q_at, s, -1e30)
            return s

        def finish(m, r, s):
            to = pl.ds(r * ROWS, ROWS)
            old = m_sc[h, m, to, :]
            new = jnp.maximum(old, jnp.max(s, axis=1, keepdims=True))
            m_sc[h, m, to, :] = new
            p = jnp.exp2((s - jnp.concatenate([new] * (keys // 128), axis=1)) * SCALE)
            factor = jnp.exp2((old - new) * SCALE)
            both = jnp.concatenate([factor, factor], axis=1)
            acc_sc[h, m, to, :] = acc_sc[h, m, to, :] * both + dot(p.astype(BF16), v)

        s = scores(*tiles[0])
        for n, tile in enumerate(tiles):
            after = scores(*tiles[n + 1]) if n + 1 < len(tiles) else None
            finish(*tile, s)
            s = after

    def half(h, carry):
        number = bounds[h]

        def pair(n, inner):
            step(h, (order[h, 2 * n], order[h, 2 * n + 1]), False)
            return inner

        lax.fori_loop(0, number // 2, pair, 0)

        @pl.when(number % 2 == 1)
        def _():
            step(h, (order[h, number - 1],), False)

        if not final:

            @pl.when(bounds[2 + h] > number)
            def _():
                step(h, (order[h, number], order[h, number + 1]), True)

        return carry

    lax.fori_loop(0, 2, half, 0)
    if final:
        for h in range(2):
            c0 = acc_sc[h, 0, :, :128] / acc_sc[h, 0, :, 128:]
            c1 = acc_sc[h, 1, :, :128] / acc_sc[h, 1, :, 128:]
            c = c0 - lam_ref[0] * c1
            c = c * lax.rsqrt(jnp.mean(c * c, axis=1, keepdims=True) + 1e-05) * gain_ref[...]
            o_ref[jnp.where(sp < blocks // 2, 1 - h, h)] = c.astype(BF16)


def attention(q, arrays, pieces, state, lambdas, gain, sp, side, final):
    half = q.shape[2]
    first = state is None
    whole = pl.BlockSpec(memory_space=pltpu.VMEM)
    scalar = pl.BlockSpec(memory_space=pltpu.SMEM)
    held = (
        jax.ShapeDtypeStruct((2, 2, half, 128), F32),
        jax.ShapeDtypeStruct((2, 2, half, 256), F32),
    )
    scratch = [
        pltpu.VMEM((len(pieces) * PIECE, arrays[0].shape[1]), BF16),
        pltpu.SemaphoreType.DMA((len(arrays),)),
        pltpu.SMEM((2, len(pieces) + 2), jnp.int32),
        pltpu.SMEM((len(pieces),), jnp.int32),
        pltpu.SMEM((4,), jnp.int32),
    ]
    if final:
        scratch = [pltpu.VMEM(h.shape, F32) for h in held] + scratch
    return pl.pallas_call(
        lambda *refs: attention_body(pieces, side, first, final, len(arrays), *refs),
        in_specs=[scalar, scalar, whole, whole]
        + [pl.BlockSpec(memory_space=pl.ANY)] * len(arrays)
        + ([] if first else [whole, whole]),
        out_specs=whole if final else (whole, whole),
        out_shape=jax.ShapeDtypeStruct((2, half, 128), BF16) if final else held,
        scratch_shapes=scratch,
        compiler_params=pltpu.CompilerParams(vmem_limit_bytes=ATTENTION_LIMIT),
        cost_estimate=cost(len(pieces)),
        name="attention",
    )(sp.reshape(1), lambdas, gain.reshape(1, 128), q, *arrays, *(() if first else state))


def spread(array, forth, back):
    half = array.shape[0] // 2
    before, behind = lax.ppermute(array, "sp", forth), lax.ppermute(array, "sp", back)
    far = lax.ppermute(before[:half], "sp", forth), lax.ppermute(behind[half:], "sp", back)
    return (before, behind), far


def attend(queries, key_rows, value_rows, lambdas, head_gain, weights, swap):
    sp_size, tp_size = lax.axis_size("sp"), lax.axis_size("tp")
    side = math.isqrt(sp_size)
    sp = lax.axis_index("sp")
    length = queries.shape[0]
    kv = jnp.concatenate([key_rows, value_rows], axis=1)
    ring = {}
    for name, dz, dx in (("z+", 1, 0), ("z-", -1, 0), ("x+", 0, 1), ("x-", 0, -1)):
        ring[name] = [
            (s, (s // side + dz) % side * side + (s % side + dx) % side) for s in range(sp_size)
        ]
    along_z, along_x = (ring["z+"], ring["z-"]), (ring["x+"], ring["x-"])
    upper, lower = kv[: length // 2], kv[length // 2 :]
    split = queries.reshape(tp_size, 2, length // (2 * tp_size), queries.shape[1])
    own = split[:, 0].reshape(length // 2, -1)
    near_u, far_u = spread(upper, *along_x)
    near_l, far_l = spread(lower, *along_z)
    other = lax.ppermute(
        split[:, 1].reshape(length // 2, -1), "sp", [(s, sp_size - 1 - s) for s in range(sp_size)]
    )
    row = jnp.concatenate([upper, *near_u, *far_u], axis=0)
    column = jnp.concatenate([lower, *near_l, *far_l], axis=0)
    near_row, far_row = spread(row, *along_z)
    near_column, far_column = spread(column, *along_x)
    steps = (0, -1, 1, 2)

    zero = jnp.zeros((2, length // 2, DH), BF16)
    q = jnp.stack([other, own])
    q = jnp.stack(
        [jnp.concatenate([q[..., :DH], zero], -1), jnp.concatenate([zero, q[..., DH:]], -1)], 1
    )
    calls = (
        ((row, column), [(0, d, 0) for d in steps] + [(d, 0, 1) for d in steps]),
        (
            near_row + near_column,
            [(e, d, 0) for e in (-1, 1) for d in steps] + [(d, e, 1) for e in (-1, 1) for d in steps],
        ),
        (far_row + far_column, [(2, d, 0) for d in steps] + [(d, 2, 1) for d in steps]),
    )
    state = None
    for n, (arrays, pieces) in enumerate(calls):
        state = attention(
            q, arrays, pieces, state, lambdas, head_gain, sp, side, n + 1 == len(calls)
        )
        if n == 0:
            weights, state = lax.optimization_barrier((weights, state))
            swapped = tuple(swap(w) for w in weights)
    return state, swapped


def project_body(h_ref, w_ref, s_ref, g_ref, d_ref, a_ref, *o_refs):
    parts = [jnp.concatenate([h_ref[n, t] for t in range(h_ref.shape[1])], axis=1) for n in range(2)]
    x = jnp.concatenate(parts, axis=0)
    attended = s_ref[...].astype(F32) + dot(x, w_ref[...])
    a_ref[...] = attended
    mean = jnp.mean(attended * attended, axis=1, keepdims=True)
    normed = (attended * lax.rsqrt(mean + 1e-06) * g_ref[...]).astype(BF16)
    pieces = stacked(normed)
    for c, o_ref in enumerate(o_refs):
        rows = dot(d_ref[c], pieces).astype(BF16)
        for h in range(SHARERS):
            o_ref[h] = rows


def stacked(x):
    wide = x.shape[1] // CUTS
    return jnp.concatenate([x[:, n * wide : (n + 1) * wide] for n in range(CUTS)], axis=0)


def project(heads, out_weight, stream, gain, dispatch):
    rows, width = stream.shape
    packed = jax.ShapeDtypeStruct((SHARERS, dispatch.shape[1], width // CUTS), BF16)
    return pl.pallas_call(
        project_body,
        out_shape=(jax.ShapeDtypeStruct((rows, width), F32),) + (packed,) * CHUNKS,
        compiler_params=pltpu.CompilerParams(vmem_limit_bytes=VMEM_LIMIT),
        cost_estimate=cost(5),
        name="project",
    )(heads, out_weight, stream, gain.reshape(1, width), dispatch)


def cost(microseconds):
    return pl.CostEstimate(flops=int(microseconds * FLOPS_US), bytes_accessed=0, transcendentals=0)


def expert_body(sets, r_any, s_any, p_any, *refs):
    weights = refs[: 3 * sets]
    o_ref, r_ref, s_ref, p_ref, x_sc, acc_sc, in_buf, down_buf, sem, small = refs[3 * sets :]
    hidden = in_buf.shape[2] // 2
    rows = s_ref.shape[0] // CUTS

    def copy(n, kind):
        if kind < 2:
            to = in_buf.at[n, :, pl.ds(kind * hidden, hidden)]
        else:
            to = down_buf.at[n // 2, pl.ds(n % 2 * hidden, hidden), :]
        return pltpu.make_async_copy(weights[3 * n + kind], to, sem.at[3 * n + kind])

    first = pltpu.make_async_copy(r_any, r_ref, small.at[0])
    second = pltpu.make_async_copy(s_any, s_ref, small.at[1])
    third = pltpu.make_async_copy(p_any, p_ref, small.at[2])
    order = [
        (2 * p + n, kind)
        for p in range(sets // 2)
        for n, kind in ((0, 0), (0, 1), (1, 0), (1, 1), (0, 2), (1, 2))
    ]
    first.start()
    second.start()
    for n, kind in order[:2]:
        copy(n, kind).start()
    first.wait()
    second.wait()
    for n, kind in order[2:]:
        copy(n, kind).start()
    third.start()
    wide = r_ref.shape[2]
    for h in range(SHARERS):
        cuts = dot(s_ref[...], r_ref[h]).astype(BF16)
        for n in range(CUTS):
            x_sc[h * rows : (h + 1) * rows, n * wide : (n + 1) * wide] = cuts[n * rows : (n + 1) * rows]
    x = x_sc[...]
    for p in range(sets // 2):
        acts = []
        for n in (2 * p, 2 * p + 1):
            copy(n, 0).wait()
            copy(n, 1).wait()
            both = dot(x, in_buf[n])
            gate, upper = both[:, :hidden], both[:, hidden:]
            acts.append((gate / (1.0 + jnp.exp(-gate)) * upper).astype(BF16))
        copy(2 * p, 2).wait()
        copy(2 * p + 1, 2).wait()
        part = dot(jnp.concatenate(acts, axis=1), down_buf[p])
        if p == 0:
            acc_sc[...] = part
        elif p + 1 < sets // 2:
            acc_sc[...] += part
        else:
            whole = (acc_sc[...] + part).astype(BF16)
            third.wait()
            for h in range(SHARERS):
                mine = whole[h * rows : (h + 1) * rows]
                o_ref[h] = dot(p_ref[...], stacked(mine)).astype(BF16)


def expert(arrived, select, place, sets):
    rows = SHARERS * select.shape[0] // CUTS
    width, hidden = sets[0][0].shape
    flat = [w for one in sets for w in one]
    return pl.pallas_call(
        lambda *refs: expert_body(len(sets), *refs),
        in_specs=[pl.BlockSpec(memory_space=pl.ANY)] * (3 + len(flat)),
        out_specs=pl.BlockSpec(memory_space=pltpu.VMEM),
        out_shape=jax.ShapeDtypeStruct(arrived.shape, BF16),
        scratch_shapes=[
            pltpu.VMEM(arrived.shape, BF16),
            pltpu.VMEM(select.shape, BF16),
            pltpu.VMEM(place.shape, BF16),
            pltpu.VMEM((rows, width), BF16),
            pltpu.VMEM((rows, width), F32),
            pltpu.VMEM((len(sets), width, 2 * hidden), BF16),
            pltpu.VMEM((len(sets) // 2, 2 * hidden, width), BF16),
            pltpu.SemaphoreType.DMA((len(flat),)),
            pltpu.SemaphoreType.DMA((3,)),
        ],
        compiler_params=pltpu.CompilerParams(vmem_limit_bytes=VMEM_LIMIT),
        cost_estimate=cost(16),
        name="expert",
    )(arrived, select, place, *flat)


def combine_body(*refs):
    r_refs, (w_ref, a_ref, o_ref) = refs[:CHUNKS], refs[CHUNKS:]
    wide = r_refs[0].shape[2]
    rows = a_ref.shape[0]
    r = jnp.concatenate(
        [sum(r_ref[h].astype(F32) for h in range(SHARERS)).astype(BF16) for r_ref in r_refs], axis=0
    )
    for n in range(CUTS):
        at = slice(n * wide, n * wide + wide)
        both = dot(w_ref[n], r)
        o_ref[:, at] = (a_ref[:, at] + (both[:rows] + both[rows:])).astype(BF16)


def combine(returned, weights, attended):
    return pl.pallas_call(
        combine_body,
        out_shape=jax.ShapeDtypeStruct(attended.shape, BF16),
        compiler_params=pltpu.CompilerParams(vmem_limit_bytes=VMEM_LIMIT),
        name="combine",
    )(*returned, weights, attended)


def moved(sp_size, tp_size, shift, flip):
    pairs = []
    for s in range(sp_size):
        for t in range(tp_size):
            y, c = t // 2, t % 2
            to = (y + shift(c)) % (tp_size // 2) * 2 + (c ^ flip)
            pairs.append((s * tp_size + t, s * tp_size + to))
    return pairs


def local(
    queries,
    key_rows,
    value_rows,
    lambdas,
    head_gain,
    out_weight,
    stream,
    ffn_gain,
    routes,
    route_weight,
    gate_weight,
    up_weight,
    down_weight,
):
    sp_size = lax.axis_size("sp")
    tp_size = lax.axis_size("tp")
    sp = lax.axis_index("sp")
    rows_local, width = stream.shape
    experts = sp_size * gate_weight.shape[0]
    top_count = routes.shape[1]
    low = sp < sp_size // 2

    mine = (gate_weight[0], up_weight[0], down_weight[0])
    along = moved(sp_size, tp_size, lambda c: 2 * c - 1, 0)
    sibling = moved(sp_size, tp_size, lambda c: 0, 1)
    passed = tuple(lax.ppermute(w, BOTH, along) for w in mine)

    slots = max(2, (rows_local * top_count * 5 + 4 * experts - 1) // (4 * experts))
    part = slots // CHUNKS
    flat = routes.reshape(-1)
    onehot = (flat[:, None] == jnp.arange(experts, dtype=jnp.int32)[None, :]).astype(BF16)
    count = flat.shape[0]
    earlier = (jnp.arange(count)[None, :] < jnp.arange(count)[:, None]).astype(BF16)
    slot = jnp.sum(dot(earlier, onehot) * onehot.astype(F32), axis=1).astype(jnp.int32)
    packed = experts * part * CUTS
    places = jnp.arange(packed, dtype=jnp.int32)

    def spots(k):
        e, j = (v.reshape(rows_local, top_count)[:, k] for v in (flat, slot))
        return [
            [jnp.where(j // part == c, (e * CUTS + n) * part + j % part, -1) for n in range(CUTS)]
            for c in range(CHUNKS)
        ]

    chosen = [spots(k) for k in range(top_count)]
    dispatch = sum(
        (places[:, None] == jnp.stack([jnp.concatenate(c) for c in at])[:, None, :]).astype(BF16)
        for at in chosen
    )
    every = jnp.arange(CHUNKS * packed, dtype=jnp.int32)
    weighted = sum(
        jnp.where(
            every
            == jnp.stack(
                [
                    sum(jnp.where(at[c][n] < 0, 0, at[c][n] + c * packed) for c in range(CHUNKS))
                    for n in range(CUTS)
                ]
            )[..., None],
            route_weight[:, k : k + 1],
            0.0,
        )
        for k, at in enumerate(chosen)
    )
    weights = jnp.concatenate(
        [weighted.astype(BF16), (weighted - lax.reduce_precision(weighted, 8, 7)).astype(BF16)], axis=1
    )
    row = jnp.arange(experts * part, dtype=jnp.int32)
    cuts = jnp.concatenate([(row // part * CUTS + n) * part + row % part for n in range(CUTS)])
    select = (cuts[:, None] == places).astype(BF16)
    place = (places[:, None] == cuts).astype(BF16)

    heads, mine_too = attend(
        queries, key_rows, value_rows, lambdas, head_gain, mine, lambda w: lax.ppermute(w, BOTH, sibling)
    )
    half = rows_local // 2
    heads = heads.reshape(2 * tp_size, half, 128)
    groups = [
        [s * tp_size + t for s in (n, sp_size - 1 - n) for t in range(tp_size)]
        for n in range(sp_size // 2)
    ]
    heads = lax.all_to_all(
        heads, BOTH, split_axis=0, concat_axis=0, tiled=True, axis_index_groups=groups
    ).reshape(2, tp_size, half, 128)
    heads = jnp.where(low, heads, heads[::-1])

    attended, *outgoing = project(heads, out_weight, stream, ffn_gain, dispatch)

    passed, outgoing = lax.optimization_barrier((passed, outgoing))
    passed_too = tuple(lax.ppermute(w, BOTH, sibling) for w in passed)
    sets = (mine, mine_too, passed, passed_too)

    ring = tp_size // 2
    members = [
        [
            s * tp_size + (y + h * (ring // SHARERS)) * 2 + c
            for h in range(SHARERS)
            for s in range(sp_size)
        ]
        for y in range(ring // SHARERS)
        for c in range(2)
    ]

    def exchange(x):
        x = x.reshape(SHARERS * experts, CUTS * part, width // CUTS)
        return lax.all_to_all(
            x, BOTH, split_axis=0, concat_axis=0, tiled=True, axis_index_groups=members
        ).reshape(SHARERS, packed, width // CUTS)

    arrived = [exchange(x) for x in outgoing]
    returned = [exchange(expert(x, select, place, sets)) for x in arrived]
    return combine(returned, weights, attended)


def solution(mesh):
    placed = (
        P("sp", "tp"),
        P("sp", "tp"),
        P("sp", "tp"),
        P("tp"),
        P(),
        P(),
        P(("sp", "tp"), None),
        P(),
        P(("sp", "tp"), None),
        P(("sp", "tp"), None),
        P("sp", None, "tp"),
        P("sp", None, "tp"),
        P("sp", "tp", None),
    )
    return jax.shard_map(
        local, mesh=mesh, in_specs=placed, out_specs=P(("sp", "tp"), None), check_vma=False
    )
```

```python
import math

import jax
import jax.numpy as jnp
from jax import lax
from jax.experimental import pallas as pl
from jax.experimental.pallas import tpu as pltpu
from jax.sharding import PartitionSpec as P


DH = 64
PIECE = 512
ROWS = 256
SCALE = DH**-0.5 * math.log2(math.e)
BOTH = ("sp", "tp")
F32 = jnp.float32
BF16 = jnp.bfloat16
VMEM_LIMIT = 58 * 1024 * 1024
ATTENTION_LIMIT = 26 * 1024 * 1024
CHUNKS = 2
CUTS = 4
SHARERS = 2
FLOPS_US = 1.0e9


def dot(a, b, dims=((1,), (0,))):
    return lax.dot_general(a, b, (dims, ((), ())), preferred_element_type=F32)


def attention_body(pieces, side, first, final, count, *refs):
    sp_ref, lam_ref, gain_ref, q_ref = refs[:4]
    kv_refs, refs = refs[4 : 4 + count], refs[4 + count :]
    if first:
        m_ref, acc_ref = None, None
    else:
        (m_ref, acc_ref), refs = refs[:2], refs[2:]
    if final:
        (o_ref, m_sc, acc_sc), refs = refs[:3], refs[3:]
    else:
        (m_sc, acc_sc), refs = refs[:2], refs[2:]
    kv, sem, order, base_at, bounds = refs[:5]
    sp = sp_ref[0]
    z, x = sp // side, sp % side
    blocks = side * side
    begin = 0
    copies = []
    for n, ref in enumerate(kv_refs):
        copies.append(pltpu.make_async_copy(ref, kv.at[pl.ds(begin, ref.shape[0])], sem.at[n]))
        begin += ref.shape[0]
    for c in copies:
        c.start()
    if first:
        m_sc[...] = jnp.full(m_sc.shape, -1e30, F32)
        acc_sc[...] = jnp.zeros(acc_sc.shape, F32)
    else:
        m_sc[...] = m_ref[...]
        acc_sc[...] = acc_ref[...]

    mine = (blocks - 1 - sp, sp)
    for n, (dz, dx, low) in enumerate(pieces):
        block = (z + dz + side) % side * side + (x + dx + side) % side
        base_at[n] = block * (2 * PIECE) + low * PIECE
        for h in range(2):
            spot = jnp.int32(0) if n == 0 else bounds[h]
            order[h, spot] = jnp.int32(n)
            bounds[h] = spot + (block < mine[h]).astype(jnp.int32)
    for h in range(2):
        spot = bounds[h]
        for n in range(len(pieces)):
            order[h, spot] = jnp.int32(n)
            spot = spot + (base_at[n] // (2 * PIECE) == mine[h]).astype(jnp.int32)
        bounds[2 + h] = spot
    for c in copies:
        c.wait()

    rows = q_ref.shape[2]

    def step(h, at, masked):
        keys = len(at) * PIECE

        def operands():
            parts = [kv[pl.ds(pl.multiple_of(p * PIECE, PIECE), PIECE), :] for p in at]
            v = jnp.concatenate([p[:, 128:] for p in parts], axis=0)
            return (
                jnp.concatenate([p[:, :128] for p in parts], axis=0),
                jnp.concatenate([v, jnp.ones((keys, 128), BF16)], axis=1),
            )

        def tile(r):
            return pl.ds(r * ROWS if isinstance(r, int) else pl.multiple_of(r * ROWS, ROWS), ROWS)

        def scores(m, r, k):
            s = dot(q_ref[h, m, tile(r), :], k, ((1,), (1,)))
            if masked:
                row = r * ROWS + lax.broadcasted_iota(jnp.int32, s.shape, 0)
                start = jnp.where(h == 0, (blocks - 1 - sp) * (2 * PIECE) + 64, sp * (2 * PIECE))
                q_at = start + lax.shift_right_logical(row, 6) * 128 + (row & 63)
                key = lax.broadcasted_iota(jnp.int32, s.shape, 1)
                key = key + jnp.where(key < PIECE, base_at[at[0]], base_at[at[-1]] - (keys - PIECE))
                s = jnp.where(key <= q_at, s, -1e30)
            return s

        def finish(m, r, s, v):
            to = tile(r)
            old = m_sc[h, m, to, :]
            new = jnp.maximum(old, jnp.max(s, axis=1, keepdims=True))
            m_sc[h, m, to, :] = new
            p = jnp.exp2((s - jnp.concatenate([new] * (keys // 128), axis=1)) * SCALE)
            factor = jnp.exp2((old - new) * SCALE)
            both = jnp.concatenate([factor, factor], axis=1)
            acc_sc[h, m, to, :] = acc_sc[h, m, to, :] * both + dot(p.astype(BF16), v)

        def run(tiles):
            k, v = operands()
            s = scores(*tiles[0], k)
            for n, at_tile in enumerate(tiles):
                after = scores(*tiles[n + 1], k) if n + 1 < len(tiles) else None
                finish(*at_tile, s, v)
                s = after

        if len(at) == 2 and not masked:
            run([(m, r) for r in range(rows // ROWS) for m in range(2)])
        else:

            def some(r, carry):
                run([(m, r) for m in range(2)])
                return carry

            lax.fori_loop(0, rows // ROWS, some, 0)

    def half(h, carry):
        number = bounds[h]

        def pair(n, inner):
            step(h, (order[h, 2 * n], order[h, 2 * n + 1]), False)
            return inner

        lax.fori_loop(0, number // 2, pair, 0)

        @pl.when(number % 2 == 1)
        def _():
            step(h, (order[h, number - 1],), False)

        if not final:

            @pl.when(bounds[2 + h] > number)
            def _():
                step(h, (order[h, number], order[h, number + 1]), True)

        return carry

    lax.fori_loop(0, 2, half, 0)
    if final:
        def close(h, carry):
            c0 = acc_sc[h, 0, :, :128] / acc_sc[h, 0, :, 128:]
            c1 = acc_sc[h, 1, :, :128] / acc_sc[h, 1, :, 128:]
            c = c0 - lam_ref[0] * c1
            c = c * lax.rsqrt(jnp.mean(c * c, axis=1, keepdims=True) + 1e-05) * gain_ref[...]
            o_ref[jnp.where(sp < blocks // 2, 1 - h, h)] = c.astype(BF16)
            return carry

        lax.fori_loop(0, 2, close, 0)


def attention(q, arrays, pieces, state, lambdas, gain, sp, side, final):
    half = q.shape[2]
    first = state is None
    whole = pl.BlockSpec(memory_space=pltpu.VMEM)
    scalar = pl.BlockSpec(memory_space=pltpu.SMEM)
    held = (
        jax.ShapeDtypeStruct((2, 2, half, 128), F32),
        jax.ShapeDtypeStruct((2, 2, half, 256), F32),
    )
    scratch = [
        pltpu.VMEM((len(pieces) * PIECE, arrays[0].shape[1]), BF16),
        pltpu.SemaphoreType.DMA((len(arrays),)),
        pltpu.SMEM((2, len(pieces) + 2), jnp.int32),
        pltpu.SMEM((len(pieces),), jnp.int32),
        pltpu.SMEM((4,), jnp.int32),
    ]
    if final:
        scratch = [pltpu.VMEM(h.shape, F32) for h in held] + scratch
    return pl.pallas_call(
        lambda *refs: attention_body(pieces, side, first, final, len(arrays), *refs),
        in_specs=[scalar, scalar, whole, whole]
        + [pl.BlockSpec(memory_space=pl.ANY)] * len(arrays)
        + ([] if first else [whole, whole]),
        out_specs=whole if final else (whole, whole),
        out_shape=jax.ShapeDtypeStruct((2, half, 128), BF16) if final else held,
        scratch_shapes=scratch,
        compiler_params=pltpu.CompilerParams(vmem_limit_bytes=ATTENTION_LIMIT),
        cost_estimate=cost(len(pieces)),
        name="attention",
    )(sp.reshape(1), lambdas, gain.reshape(1, 128), q, *arrays, *(() if first else state))


def spread(array, forth, back):
    half = array.shape[0] // 2
    before, behind = lax.ppermute(array, "sp", forth), lax.ppermute(array, "sp", back)
    far = lax.ppermute(before[:half], "sp", forth), lax.ppermute(behind[half:], "sp", back)
    return (before, behind), far


def attend(queries, key_rows, value_rows, lambdas, head_gain, weights, swap):
    sp_size, tp_size = lax.axis_size("sp"), lax.axis_size("tp")
    side = math.isqrt(sp_size)
    sp = lax.axis_index("sp")
    length = queries.shape[0]
    kv = jnp.concatenate([key_rows, value_rows], axis=1)
    ring = {}
    for name, dz, dx in (("z+", 1, 0), ("z-", -1, 0), ("x+", 0, 1), ("x-", 0, -1)):
        ring[name] = [
            (s, (s // side + dz) % side * side + (s % side + dx) % side) for s in range(sp_size)
        ]
    along_z, along_x = (ring["z+"], ring["z-"]), (ring["x+"], ring["x-"])
    upper, lower = kv[: length // 2], kv[length // 2 :]
    split = queries.reshape(tp_size, 2, length // (2 * tp_size), queries.shape[1])
    own = split[:, 0].reshape(length // 2, -1)
    near_u, far_u = spread(upper, *along_x)
    near_l, far_l = spread(lower, *along_z)
    other = lax.ppermute(
        split[:, 1].reshape(length // 2, -1), "sp", [(s, sp_size - 1 - s) for s in range(sp_size)]
    )
    row = jnp.concatenate([upper, *near_u, *far_u], axis=0)
    column = jnp.concatenate([lower, *near_l, *far_l], axis=0)
    near_row, far_row = spread(row, *along_z)
    near_column, far_column = spread(column, *along_x)
    steps = (0, -1, 1, 2)

    zero = jnp.zeros((2, length // 2, DH), BF16)
    q = jnp.stack([other, own])
    q = jnp.stack(
        [jnp.concatenate([q[..., :DH], zero], -1), jnp.concatenate([zero, q[..., DH:]], -1)], 1
    )
    calls = (
        ((row, column), [(0, d, 0) for d in steps] + [(d, 0, 1) for d in steps]),
        (
            near_row + near_column,
            [(e, d, 0) for e in (-1, 1) for d in steps] + [(d, e, 1) for e in (-1, 1) for d in steps],
        ),
        (far_row + far_column, [(2, d, 0) for d in steps] + [(d, 2, 1) for d in steps]),
    )
    state = None
    for n, (arrays, pieces) in enumerate(calls):
        state = attention(
            q, arrays, pieces, state, lambdas, head_gain, sp, side, n + 1 == len(calls)
        )
        if n == 0:
            weights, state = lax.optimization_barrier((weights, state))
            swapped = tuple(swap(w) for w in weights)
    return state, swapped


def project_body(h_ref, w_ref, s_ref, g_ref, d_ref, a_ref, *o_refs):
    parts = [jnp.concatenate([h_ref[n, t] for t in range(h_ref.shape[1])], axis=1) for n in range(2)]
    x = jnp.concatenate(parts, axis=0)
    attended = s_ref[...].astype(F32) + dot(x, w_ref[...])
    a_ref[...] = attended
    mean = jnp.mean(attended * attended, axis=1, keepdims=True)
    normed = (attended * lax.rsqrt(mean + 1e-06) * g_ref[...]).astype(BF16)
    pieces = stacked(normed)
    for c, o_ref in enumerate(o_refs):
        rows = dot(d_ref[c], pieces).astype(BF16)
        for h in range(SHARERS):
            o_ref[h] = rows


def stacked(x):
    wide = x.shape[1] // CUTS
    return jnp.concatenate([x[:, n * wide : (n + 1) * wide] for n in range(CUTS)], axis=0)


def project(heads, out_weight, stream, gain, dispatch):
    rows, width = stream.shape
    packed = jax.ShapeDtypeStruct((SHARERS, dispatch.shape[1], width // CUTS), BF16)
    return pl.pallas_call(
        project_body,
        out_shape=(jax.ShapeDtypeStruct((rows, width), F32),) + (packed,) * CHUNKS,
        compiler_params=pltpu.CompilerParams(vmem_limit_bytes=VMEM_LIMIT),
        cost_estimate=cost(5),
        name="project",
    )(heads, out_weight, stream, gain.reshape(1, width), dispatch)


def cost(microseconds):
    return pl.CostEstimate(flops=int(microseconds * FLOPS_US), bytes_accessed=0, transcendentals=0)


def expert_body(sets, r_any, s_any, p_any, *refs):
    weights = refs[: 3 * sets]
    o_ref, r_ref, s_ref, p_ref, x_sc, act_sc, acc_sc, in_buf, down_buf, sem, small = refs[3 * sets :]
    hidden = in_buf.shape[2] // 2
    rows = s_ref.shape[0] // CUTS

    def copy(n, kind):
        if kind < 2:
            to = in_buf.at[n, :, pl.ds(kind * hidden, hidden)]
        else:
            to = down_buf.at[n // 2, pl.ds(n % 2 * hidden, hidden), :]
        return pltpu.make_async_copy(weights[3 * n + kind], to, sem.at[3 * n + kind])

    def share(h):
        return pl.ds(pl.multiple_of(h * rows, 16), rows)

    def landed(kind, n):
        if kind < 2:
            to = in_buf.at[n, :, pl.ds(kind * hidden, hidden)]
        else:
            to = down_buf.at[n // 2, pl.ds(pl.multiple_of(n % 2 * hidden, 128), hidden), :]
        pltpu.make_async_copy(weights[kind], to, sem.at[3 * n + kind]).wait()

    first = pltpu.make_async_copy(r_any, r_ref, small.at[0])
    second = pltpu.make_async_copy(s_any, s_ref, small.at[1])
    third = pltpu.make_async_copy(p_any, p_ref, small.at[2])
    order = [
        (2 * p + n, kind)
        for p in range(sets // 2)
        for n, kind in ((0, 0), (0, 1), (1, 0), (1, 1), (0, 2), (1, 2))
    ]
    first.start()
    second.start()
    for n, kind in order[:2]:
        copy(n, kind).start()
    first.wait()
    second.wait()
    for n, kind in order[2:]:
        copy(n, kind).start()
    third.start()
    wide = r_ref.shape[2]

    def unpack(h, carry):
        cuts = dot(s_ref[...], r_ref[h]).astype(BF16)
        for n in range(CUTS):
            x_sc[share(h), n * wide : (n + 1) * wide] = cuts[n * rows : (n + 1) * rows]
        return carry

    lax.fori_loop(0, SHARERS, unpack, 0)

    def pair(p, carry):
        def one(v, inner):
            n = 2 * p + v
            for kind in range(2):
                landed(kind, n)
            both = dot(x_sc[...], in_buf[n])
            gate, upper = both[:, :hidden], both[:, hidden:]
            act = (gate / (1.0 + jnp.exp(-gate)) * upper).astype(BF16)
            act_sc[:, pl.ds(pl.multiple_of(v * hidden, 128), hidden)] = act
            return inner

        lax.fori_loop(0, 2, one, 0)
        landed(2, 2 * p)
        landed(2, 2 * p + 1)
        acc_sc[...] += dot(act_sc[...], down_buf[p])
        return carry

    acc_sc[...] = jnp.zeros(acc_sc.shape, F32)
    lax.fori_loop(0, sets // 2, pair, 0)
    third.wait()

    def repack(h, carry):
        o_ref[h] = dot(p_ref[...], stacked(acc_sc[share(h), :].astype(BF16))).astype(BF16)
        return carry

    lax.fori_loop(0, SHARERS, repack, 0)


def expert(arrived, select, place, sets):
    rows = SHARERS * select.shape[0] // CUTS
    width, hidden = sets[0][0].shape
    flat = [w for one in sets for w in one]
    return pl.pallas_call(
        lambda *refs: expert_body(len(sets), *refs),
        in_specs=[pl.BlockSpec(memory_space=pl.ANY)] * (3 + len(flat)),
        out_specs=pl.BlockSpec(memory_space=pltpu.VMEM),
        out_shape=jax.ShapeDtypeStruct(arrived.shape, BF16),
        scratch_shapes=[
            pltpu.VMEM(arrived.shape, BF16),
            pltpu.VMEM(select.shape, BF16),
            pltpu.VMEM(place.shape, BF16),
            pltpu.VMEM((rows, width), BF16),
            pltpu.VMEM((rows, 2 * hidden), BF16),
            pltpu.VMEM((rows, width), F32),
            pltpu.VMEM((len(sets), width, 2 * hidden), BF16),
            pltpu.VMEM((len(sets) // 2, 2 * hidden, width), BF16),
            pltpu.SemaphoreType.DMA((len(flat),)),
            pltpu.SemaphoreType.DMA((3,)),
        ],
        compiler_params=pltpu.CompilerParams(vmem_limit_bytes=VMEM_LIMIT),
        cost_estimate=cost(16),
        name="expert",
    )(arrived, select, place, *flat)


def combine_body(*refs):
    r_refs, (w_ref, a_ref, o_ref, r_sc) = refs[:CHUNKS], refs[CHUNKS:]
    wide = r_refs[0].shape[2]
    rows = a_ref.shape[0]
    for c, r_ref in enumerate(r_refs):
        total = sum(r_ref[h].astype(F32) for h in range(SHARERS))
        r_sc[c * total.shape[0] : (c + 1) * total.shape[0], :] = total.astype(BF16)

    def one(n, carry):
        at = pl.ds(pl.multiple_of(n * wide, 128), wide)
        both = dot(w_ref[n], r_sc[...])
        o_ref[:, at] = (a_ref[:, at] + (both[:rows] + both[rows:])).astype(BF16)
        return carry

    lax.fori_loop(0, CUTS, one, 0)


def combine(returned, weights, attended):
    return pl.pallas_call(
        combine_body,
        out_shape=jax.ShapeDtypeStruct(attended.shape, BF16),
        scratch_shapes=[pltpu.VMEM((weights.shape[2], attended.shape[1] // CUTS), BF16)],
        compiler_params=pltpu.CompilerParams(vmem_limit_bytes=VMEM_LIMIT),
        name="combine",
    )(*returned, weights, attended)


def moved(sp_size, tp_size, shift, flip):
    pairs = []
    for s in range(sp_size):
        for t in range(tp_size):
            y, c = t // 2, t % 2
            to = (y + shift(c)) % (tp_size // 2) * 2 + (c ^ flip)
            pairs.append((s * tp_size + t, s * tp_size + to))
    return pairs


def local(
    queries,
    key_rows,
    value_rows,
    lambdas,
    head_gain,
    out_weight,
    stream,
    ffn_gain,
    routes,
    route_weight,
    gate_weight,
    up_weight,
    down_weight,
):
    sp_size = lax.axis_size("sp")
    tp_size = lax.axis_size("tp")
    sp = lax.axis_index("sp")
    rows_local, width = stream.shape
    experts = sp_size * gate_weight.shape[0]
    top_count = routes.shape[1]
    low = sp < sp_size // 2

    mine = (gate_weight[0], up_weight[0], down_weight[0])
    along = moved(sp_size, tp_size, lambda c: 2 * c - 1, 0)
    sibling = moved(sp_size, tp_size, lambda c: 0, 1)
    passed = []
    for w in mine:
        passed.append(lax.ppermute(w, BOTH, along))
    passed = tuple(passed)

    slots = max(2, (rows_local * top_count * 5 + 4 * experts - 1) // (4 * experts))
    part = slots // CHUNKS
    flat = routes.reshape(-1)
    onehot = (flat[:, None] == jnp.arange(experts, dtype=jnp.int32)[None, :]).astype(BF16)
    count = flat.shape[0]
    earlier = (jnp.arange(count)[None, :] < jnp.arange(count)[:, None]).astype(BF16)
    slot = jnp.sum(dot(earlier, onehot) * onehot.astype(F32), axis=1).astype(jnp.int32)
    packed = experts * part * CUTS
    places = jnp.arange(packed, dtype=jnp.int32)

    def spots(k):
        e, j = (v.reshape(rows_local, top_count)[:, k] for v in (flat, slot))
        return [
            [jnp.where(j // part == c, (e * CUTS + n) * part + j % part, -1) for n in range(CUTS)]
            for c in range(CHUNKS)
        ]

    chosen = [spots(k) for k in range(top_count)]
    dispatch = sum(
        (places[:, None] == jnp.stack([jnp.concatenate(c) for c in at])[:, None, :]).astype(BF16)
        for at in chosen
    )
    every = jnp.arange(CHUNKS * packed, dtype=jnp.int32)
    weighted = sum(
        jnp.where(
            every
            == jnp.stack(
                [
                    sum(jnp.where(at[c][n] < 0, 0, at[c][n] + c * packed) for c in range(CHUNKS))
                    for n in range(CUTS)
                ]
            )[..., None],
            route_weight[:, k : k + 1],
            0.0,
        )
        for k, at in enumerate(chosen)
    )
    weights = jnp.concatenate(
        [weighted.astype(BF16), (weighted - lax.reduce_precision(weighted, 8, 7)).astype(BF16)], axis=1
    )
    row = jnp.arange(experts * part, dtype=jnp.int32)
    cuts = jnp.concatenate([(row // part * CUTS + n) * part + row % part for n in range(CUTS)])
    select = (cuts[:, None] == places).astype(BF16)
    place = (places[:, None] == cuts).astype(BF16)

    heads, mine_too = attend(
        queries, key_rows, value_rows, lambdas, head_gain, mine, lambda w: lax.ppermute(w, BOTH, sibling)
    )
    half = rows_local // 2
    heads = heads.reshape(2 * tp_size, half, 128)
    groups = [
        [s * tp_size + t for s in (n, sp_size - 1 - n) for t in range(tp_size)]
        for n in range(sp_size // 2)
    ]
    heads = lax.all_to_all(
        heads, BOTH, split_axis=0, concat_axis=0, tiled=True, axis_index_groups=groups
    ).reshape(2, tp_size, half, 128)
    heads = jnp.where(low, heads, heads[::-1])

    attended, *outgoing = project(heads, out_weight, stream, ffn_gain, dispatch)

    passed, outgoing = lax.optimization_barrier((passed, outgoing))
    passed_too = tuple(lax.ppermute(w, BOTH, sibling) for w in passed)
    sets = (mine, mine_too, passed, passed_too)

    ring = tp_size // 2
    members = [
        [
            s * tp_size + (y + h * (ring // SHARERS)) * 2 + c
            for h in range(SHARERS)
            for s in range(sp_size)
        ]
        for y in range(ring // SHARERS)
        for c in range(2)
    ]

    def exchange(x):
        x = x.reshape(SHARERS * experts, CUTS * part, width // CUTS)
        return lax.all_to_all(
            x, BOTH, split_axis=0, concat_axis=0, tiled=True, axis_index_groups=members
        ).reshape(SHARERS, packed, width // CUTS)

    arrived = [exchange(x) for x in outgoing]
    returned = [exchange(expert(x, select, place, sets)) for x in arrived]
    return combine(returned, weights, attended)


def solution(mesh):
    placed = (
        P("sp", "tp"),
        P("sp", "tp"),
        P("sp", "tp"),
        P("tp"),
        P(),
        P(),
        P(("sp", "tp"), None),
        P(),
        P(("sp", "tp"), None),
        P(("sp", "tp"), None),
        P("sp", None, "tp"),
        P("sp", None, "tp"),
        P("sp", "tp", None),
    )
    return jax.shard_map(
        local, mesh=mesh, in_specs=placed, out_specs=P(("sp", "tp"), None), check_vma=False
    )
```

```python
import math

import jax
import jax.numpy as jnp
from jax import lax
from jax.experimental import pallas as pl
from jax.experimental.pallas import tpu as pltpu
from jax.sharding import PartitionSpec as P


DH = 64
PIECE = 512
ROWS = 256
SCALE = DH**-0.5 * math.log2(math.e)
BOTH = ("sp", "tp")
F32 = jnp.float32
BF16 = jnp.bfloat16
VMEM_LIMIT = 58 * 1024 * 1024
ATTENTION_LIMIT = 26 * 1024 * 1024
CHUNKS = 2
CUTS = 4
SHARERS = 2
FLOPS_US = 1.0e9


def dot(a, b, dims=((1,), (0,))):
    return lax.dot_general(a, b, (dims, ((), ())), preferred_element_type=F32)


def attention_body(pieces, side, first, final, count, *refs):
    sp_ref, lam_ref, gain_ref, q_ref = refs[:4]
    kv_refs, refs = refs[4 : 4 + count], refs[4 + count :]
    if first:
        m_ref, acc_ref = None, None
    else:
        (m_ref, acc_ref), refs = refs[:2], refs[2:]
    if final:
        (o_ref, m_sc, acc_sc), refs = refs[:3], refs[3:]
    else:
        (m_sc, acc_sc), refs = refs[:2], refs[2:]
    kv, sem, order, base_at, bounds = refs[:5]
    sp = sp_ref[0]
    z, x = sp // side, sp % side
    blocks = side * side
    begin = 0
    copies = []
    for n, ref in enumerate(kv_refs):
        copies.append(pltpu.make_async_copy(ref, kv.at[pl.ds(begin, ref.shape[0])], sem.at[n]))
        begin += ref.shape[0]
    for c in copies:
        c.start()
    if first:
        m_sc[...] = jnp.full(m_sc.shape, -1e30, F32)
        acc_sc[...] = jnp.zeros(acc_sc.shape, F32)
    else:
        m_sc[...] = m_ref[...]
        acc_sc[...] = acc_ref[...]

    mine = (blocks - 1 - sp, sp)
    for n, (dz, dx, low) in enumerate(pieces):
        block = (z + dz + side) % side * side + (x + dx + side) % side
        base_at[n] = block * (2 * PIECE) + low * PIECE
        for h in range(2):
            spot = jnp.int32(0) if n == 0 else bounds[h]
            order[h, spot] = jnp.int32(n)
            bounds[h] = spot + (block < mine[h]).astype(jnp.int32)
    for h in range(2):
        spot = bounds[h]
        for n in range(len(pieces)):
            order[h, spot] = jnp.int32(n)
            spot = spot + (base_at[n] // (2 * PIECE) == mine[h]).astype(jnp.int32)
        bounds[2 + h] = spot
    for c in copies:
        c.wait()

    rows = q_ref.shape[2]

    def step(h, at, masked):
        keys = len(at) * PIECE

        def operands():
            parts = [kv[pl.ds(pl.multiple_of(p * PIECE, PIECE), PIECE), :] for p in at]
            v = jnp.concatenate([p[:, 128:] for p in parts], axis=0)
            return (
                jnp.concatenate([p[:, :128] for p in parts], axis=0),
                jnp.concatenate([v, jnp.ones((keys, 128), BF16)], axis=1),
            )

        def tile(r):
            return pl.ds(r * ROWS if isinstance(r, int) else pl.multiple_of(r * ROWS, ROWS), ROWS)

        def scores(m, r, k):
            s = dot(q_ref[h, m, tile(r), :], k, ((1,), (1,)))
            if masked:
                row = r * ROWS + lax.broadcasted_iota(jnp.int32, s.shape, 0)
                start = jnp.where(h == 0, (blocks - 1 - sp) * (2 * PIECE) + 64, sp * (2 * PIECE))
                q_at = start + lax.shift_right_logical(row, 6) * 128 + (row & 63)
                key = lax.broadcasted_iota(jnp.int32, s.shape, 1)
                key = key + jnp.where(key < PIECE, base_at[at[0]], base_at[at[-1]] - (keys - PIECE))
                s = jnp.where(key <= q_at, s, -1e30)
            return s

        def finish(m, r, s, v):
            to = tile(r)
            old = m_sc[h, m, to, :]
            new = jnp.maximum(old, jnp.max(s, axis=1, keepdims=True))
            m_sc[h, m, to, :] = new
            p = jnp.exp2((s - jnp.concatenate([new] * (keys // 128), axis=1)) * SCALE)
            factor = jnp.exp2((old - new) * SCALE)
            both = jnp.concatenate([factor, factor], axis=1)
            acc_sc[h, m, to, :] = acc_sc[h, m, to, :] * both + dot(p.astype(BF16), v)

        def run(tiles):
            k, v = operands()
            s = scores(*tiles[0], k)
            for n, at_tile in enumerate(tiles):
                after = scores(*tiles[n + 1], k) if n + 1 < len(tiles) else None
                finish(*at_tile, s, v)
                s = after

        if len(at) == 2 and not masked:
            run([(m, r) for r in range(rows // ROWS) for m in range(2)])
        else:

            def some(t, carry):
                run([(t % 2, t // 2)])
                return carry

            lax.fori_loop(0, 2 * rows // ROWS, some, 0)

    def half(h, carry):
        number = bounds[h]

        def pair(n, inner):
            step(h, (order[h, 2 * n], order[h, 2 * n + 1]), False)
            return inner

        lax.fori_loop(0, number // 2, pair, 0)

        @pl.when(number % 2 == 1)
        def _():
            step(h, (order[h, number - 1],), False)

        if not final:

            @pl.when(bounds[2 + h] > number)
            def _():
                step(h, (order[h, number], order[h, number + 1]), True)

        return carry

    lax.fori_loop(0, 2, half, 0)
    if final:
        def close(h, carry):
            c0 = acc_sc[h, 0, :, :128] / acc_sc[h, 0, :, 128:]
            c1 = acc_sc[h, 1, :, :128] / acc_sc[h, 1, :, 128:]
            c = c0 - lam_ref[0] * c1
            c = c * lax.rsqrt(jnp.mean(c * c, axis=1, keepdims=True) + 1e-05) * gain_ref[...]
            o_ref[jnp.where(sp < blocks // 2, 1 - h, h)] = c.astype(BF16)
            return carry

        lax.fori_loop(0, 2, close, 0)


def attention(q, arrays, pieces, state, lambdas, gain, sp, side, final):
    half = q.shape[2]
    first = state is None
    whole = pl.BlockSpec(memory_space=pltpu.VMEM)
    scalar = pl.BlockSpec(memory_space=pltpu.SMEM)
    held = (
        jax.ShapeDtypeStruct((2, 2, half, 128), F32),
        jax.ShapeDtypeStruct((2, 2, half, 256), F32),
    )
    scratch = [
        pltpu.VMEM((len(pieces) * PIECE, arrays[0].shape[1]), BF16),
        pltpu.SemaphoreType.DMA((len(arrays),)),
        pltpu.SMEM((2, len(pieces) + 2), jnp.int32),
        pltpu.SMEM((len(pieces),), jnp.int32),
        pltpu.SMEM((4,), jnp.int32),
    ]
    if final:
        scratch = [pltpu.VMEM(h.shape, F32) for h in held] + scratch
    return pl.pallas_call(
        lambda *refs: attention_body(pieces, side, first, final, len(arrays), *refs),
        in_specs=[scalar, scalar, whole, whole]
        + [pl.BlockSpec(memory_space=pl.ANY)] * len(arrays)
        + ([] if first else [whole, whole]),
        out_specs=whole if final else (whole, whole),
        out_shape=jax.ShapeDtypeStruct((2, half, 128), BF16) if final else held,
        scratch_shapes=scratch,
        compiler_params=pltpu.CompilerParams(vmem_limit_bytes=ATTENTION_LIMIT),
        cost_estimate=cost(len(pieces)),
        name="attention",
    )(sp.reshape(1), lambdas, gain.reshape(1, 128), q, *arrays, *(() if first else state))


def spread(array, forth, back):
    half = array.shape[0] // 2
    before, behind = lax.ppermute(array, "sp", forth), lax.ppermute(array, "sp", back)
    far = lax.ppermute(before[:half], "sp", forth), lax.ppermute(behind[half:], "sp", back)
    return (before, behind), far


def attend(queries, key_rows, value_rows, lambdas, head_gain, weights, swap):
    sp_size, tp_size = lax.axis_size("sp"), lax.axis_size("tp")
    side = math.isqrt(sp_size)
    sp = lax.axis_index("sp")
    length = queries.shape[0]
    kv = jnp.concatenate([key_rows, value_rows], axis=1)
    ring = {}
    for name, dz, dx in (("z+", 1, 0), ("z-", -1, 0), ("x+", 0, 1), ("x-", 0, -1)):
        ring[name] = [
            (s, (s // side + dz) % side * side + (s % side + dx) % side) for s in range(sp_size)
        ]
    along_z, along_x = (ring["z+"], ring["z-"]), (ring["x+"], ring["x-"])
    upper, lower = kv[: length // 2], kv[length // 2 :]
    split = queries.reshape(tp_size, 2, length // (2 * tp_size), queries.shape[1])
    own = split[:, 0].reshape(length // 2, -1)
    near_u, far_u = spread(upper, *along_x)
    near_l, far_l = spread(lower, *along_z)
    other = lax.ppermute(
        split[:, 1].reshape(length // 2, -1), "sp", [(s, sp_size - 1 - s) for s in range(sp_size)]
    )
    row = jnp.concatenate([upper, *near_u, *far_u], axis=0)
    column = jnp.concatenate([lower, *near_l, *far_l], axis=0)
    near_row, far_row = spread(row, *along_z)
    near_column, far_column = spread(column, *along_x)
    steps = (0, -1, 1, 2)

    zero = jnp.zeros((2, length // 2, DH), BF16)
    q = jnp.stack([other, own])
    q = jnp.stack(
        [jnp.concatenate([q[..., :DH], zero], -1), jnp.concatenate([zero, q[..., DH:]], -1)], 1
    )
    calls = (
        ((row, column), [(0, d, 0) for d in steps] + [(d, 0, 1) for d in steps]),
        (
            near_row + near_column,
            [(e, d, 0) for e in (-1, 1) for d in steps] + [(d, e, 1) for e in (-1, 1) for d in steps],
        ),
        (far_row + far_column, [(2, d, 0) for d in steps] + [(d, 2, 1) for d in steps]),
    )
    state = None
    for n, (arrays, pieces) in enumerate(calls):
        state = attention(
            q, arrays, pieces, state, lambdas, head_gain, sp, side, n + 1 == len(calls)
        )
        if n == 0:
            weights, state = lax.optimization_barrier((weights, state))
            swapped = tuple(swap(w) for w in weights)
    return state, swapped


def project_body(h_ref, w_ref, s_ref, g_ref, d_ref, a_ref, *o_refs):
    parts = [jnp.concatenate([h_ref[n, t] for t in range(h_ref.shape[1])], axis=1) for n in range(2)]
    x = jnp.concatenate(parts, axis=0)
    attended = s_ref[...].astype(F32) + dot(x, w_ref[...])
    a_ref[...] = attended
    mean = jnp.mean(attended * attended, axis=1, keepdims=True)
    normed = (attended * lax.rsqrt(mean + 1e-06) * g_ref[...]).astype(BF16)
    pieces = stacked(normed)
    for c, o_ref in enumerate(o_refs):
        rows = dot(d_ref[c], pieces).astype(BF16)
        for h in range(SHARERS):
            o_ref[h] = rows


def stacked(x):
    wide = x.shape[1] // CUTS
    return jnp.concatenate([x[:, n * wide : (n + 1) * wide] for n in range(CUTS)], axis=0)


def project(heads, out_weight, stream, gain, dispatch):
    rows, width = stream.shape
    packed = jax.ShapeDtypeStruct((SHARERS, dispatch.shape[1], width // CUTS), BF16)
    return pl.pallas_call(
        project_body,
        out_shape=(jax.ShapeDtypeStruct((rows, width), F32),) + (packed,) * CHUNKS,
        compiler_params=pltpu.CompilerParams(vmem_limit_bytes=VMEM_LIMIT),
        cost_estimate=cost(5),
        name="project",
    )(heads, out_weight, stream, gain.reshape(1, width), dispatch)


def cost(microseconds):
    return pl.CostEstimate(flops=int(microseconds * FLOPS_US), bytes_accessed=0, transcendentals=0)


def expert_body(sizes, r_any, s_any, p_any, *refs):
    sets = len(sizes)
    flat, weights = refs, []
    for size in sizes:
        weights.append((flat[0], flat[1], flat[2:size]))
        flat = flat[size:]
    o_ref, r_ref, s_ref, p_ref, x_sc, act_sc, acc_sc, in_buf, down_buf, sem, small = flat
    hidden = in_buf.shape[2] // 2
    rows = s_ref.shape[0] // CUTS

    def start(n, kind):
        if kind < 2:
            to = in_buf.at[n, :, pl.ds(kind * hidden, hidden)]
            pltpu.make_async_copy(weights[n][kind], to, sem.at[3 * n + kind]).start()
        else:
            begin = n % 2 * hidden
            for piece in weights[n][2]:
                to = down_buf.at[n // 2, pl.ds(begin, piece.shape[0]), :]
                pltpu.make_async_copy(piece, to, sem.at[3 * n + 2]).start()
                begin += piece.shape[0]

    def share(h):
        return pl.ds(pl.multiple_of(h * rows, 16), rows)

    def landed(kind, n):
        if kind < 2:
            to = in_buf.at[n, :, pl.ds(kind * hidden, hidden)]
        else:
            to = down_buf.at[n // 2, pl.ds(pl.multiple_of(n % 2 * hidden, 128), hidden), :]
        pltpu.make_async_copy((weights[0][0], weights[0][1], weights[0][2][0])[kind], to, sem.at[3 * n + kind]).wait()

    first = pltpu.make_async_copy(r_any, r_ref, small.at[0])
    second = pltpu.make_async_copy(s_any, s_ref, small.at[1])
    third = pltpu.make_async_copy(p_any, p_ref, small.at[2])
    order = [
        (2 * p + n, kind)
        for p in range(sets // 2)
        for n, kind in ((0, 0), (0, 1), (1, 0), (1, 1), (0, 2), (1, 2))
    ]
    first.start()
    second.start()
    for n, kind in order[:2]:
        start(n, kind)
    first.wait()
    second.wait()
    for n, kind in order[2:]:
        start(n, kind)
    third.start()
    wide = r_ref.shape[2]

    def unpack(h, carry):
        cuts = dot(s_ref[...], r_ref[h]).astype(BF16)
        for n in range(CUTS):
            x_sc[share(h), n * wide : (n + 1) * wide] = cuts[n * rows : (n + 1) * rows]
        return carry

    lax.fori_loop(0, SHARERS, unpack, 0)

    def pair(p, carry):
        def one(v, inner):
            n = 2 * p + v
            for kind in range(2):
                landed(kind, n)
            both = dot(x_sc[...], in_buf[n])
            gate, upper = both[:, :hidden], both[:, hidden:]
            act = (gate / (1.0 + jnp.exp(-gate)) * upper).astype(BF16)
            act_sc[:, pl.ds(pl.multiple_of(v * hidden, 128), hidden)] = act
            return inner

        lax.fori_loop(0, 2, one, 0)
        landed(2, 2 * p)
        landed(2, 2 * p + 1)
        acc_sc[...] += dot(act_sc[...], down_buf[p])
        return carry

    acc_sc[...] = jnp.zeros(acc_sc.shape, F32)
    lax.fori_loop(0, sets // 2, pair, 0)
    third.wait()

    def repack(h, carry):
        o_ref[h] = dot(p_ref[...], stacked(acc_sc[share(h), :].astype(BF16))).astype(BF16)
        return carry

    lax.fori_loop(0, SHARERS, repack, 0)


def expert(arrived, select, place, sets):
    rows = SHARERS * select.shape[0] // CUTS
    width, hidden = sets[0][0].shape
    flat = [w for one in sets for w in one]
    return pl.pallas_call(
        lambda *refs: expert_body([len(one) for one in sets], *refs),
        in_specs=[pl.BlockSpec(memory_space=pl.ANY)] * (3 + len(flat)),
        out_specs=pl.BlockSpec(memory_space=pltpu.VMEM),
        out_shape=jax.ShapeDtypeStruct(arrived.shape, BF16),
        scratch_shapes=[
            pltpu.VMEM(arrived.shape, BF16),
            pltpu.VMEM(select.shape, BF16),
            pltpu.VMEM(place.shape, BF16),
            pltpu.VMEM((rows, width), BF16),
            pltpu.VMEM((rows, 2 * hidden), BF16),
            pltpu.VMEM((rows, width), F32),
            pltpu.VMEM((len(sets), width, 2 * hidden), BF16),
            pltpu.VMEM((len(sets) // 2, 2 * hidden, width), BF16),
            pltpu.SemaphoreType.DMA((3 * len(sets),)),
            pltpu.SemaphoreType.DMA((3,)),
        ],
        compiler_params=pltpu.CompilerParams(vmem_limit_bytes=VMEM_LIMIT),
        cost_estimate=cost(16),
        name="expert",
    )(arrived, select, place, *flat)


def combine_body(*refs):
    r_refs, (w_ref, a_ref, o_ref, r_sc) = refs[:CHUNKS], refs[CHUNKS:]
    wide = r_refs[0].shape[2]
    rows = a_ref.shape[0]
    for c, r_ref in enumerate(r_refs):
        total = sum(r_ref[h].astype(F32) for h in range(SHARERS))
        r_sc[c * total.shape[0] : (c + 1) * total.shape[0], :] = total.astype(BF16)

    def one(n, carry):
        at = pl.ds(pl.multiple_of(n * wide, 128), wide)
        both = dot(w_ref[n], r_sc[...])
        o_ref[:, at] = (a_ref[:, at] + (both[:rows] + both[rows:])).astype(BF16)
        return carry

    lax.fori_loop(0, CUTS, one, 0)


def combine(returned, weights, attended):
    return pl.pallas_call(
        combine_body,
        out_shape=jax.ShapeDtypeStruct(attended.shape, BF16),
        scratch_shapes=[pltpu.VMEM((weights.shape[2], attended.shape[1] // CUTS), BF16)],
        compiler_params=pltpu.CompilerParams(vmem_limit_bytes=VMEM_LIMIT),
        name="combine",
    )(*returned, weights, attended)


def moved(sp_size, tp_size, shift, flip):
    pairs = []
    for s in range(sp_size):
        for t in range(tp_size):
            y, c = t // 2, t % 2
            to = (y + shift(c)) % (tp_size // 2) * 2 + (c ^ flip)
            pairs.append((s * tp_size + t, s * tp_size + to))
    return pairs


def local(
    queries,
    key_rows,
    value_rows,
    lambdas,
    head_gain,
    out_weight,
    stream,
    ffn_gain,
    routes,
    route_weight,
    gate_weight,
    up_weight,
    down_weight,
):
    sp_size = lax.axis_size("sp")
    tp_size = lax.axis_size("tp")
    sp = lax.axis_index("sp")
    rows_local, width = stream.shape
    experts = sp_size * gate_weight.shape[0]
    top_count = routes.shape[1]
    low = sp < sp_size // 2

    mine = (gate_weight[0], up_weight[0], down_weight[0])
    along = moved(sp_size, tp_size, lambda c: 2 * c - 1, 0)
    sibling = moved(sp_size, tp_size, lambda c: 0, 1)
    passed = []
    gate, up, down = mine
    later = down.shape[0] // 2
    for w in (gate, up, down[:later]):
        passed.append(lax.ppermute(w, BOTH, along))
    passed = tuple(passed)

    slots = max(2, (rows_local * top_count * 5 + 4 * experts - 1) // (4 * experts))
    part = slots // CHUNKS
    flat = routes.reshape(-1)
    onehot = (flat[:, None] == jnp.arange(experts, dtype=jnp.int32)[None, :]).astype(BF16)
    count = flat.shape[0]
    earlier = (jnp.arange(count)[None, :] < jnp.arange(count)[:, None]).astype(BF16)
    slot = jnp.sum(dot(earlier, onehot) * onehot.astype(F32), axis=1).astype(jnp.int32)
    packed = experts * part * CUTS
    places = jnp.arange(packed, dtype=jnp.int32)

    def spots(k):
        e, j = (v.reshape(rows_local, top_count)[:, k] for v in (flat, slot))
        return [
            [jnp.where(j // part == c, (e * CUTS + n) * part + j % part, -1) for n in range(CUTS)]
            for c in range(CHUNKS)
        ]

    chosen = [spots(k) for k in range(top_count)]
    dispatch = sum(
        (places[:, None] == jnp.stack([jnp.concatenate(c) for c in at])[:, None, :]).astype(BF16)
        for at in chosen
    )
    every = jnp.arange(CHUNKS * packed, dtype=jnp.int32)
    weighted = sum(
        jnp.where(
            every
            == jnp.stack(
                [
                    sum(jnp.where(at[c][n] < 0, 0, at[c][n] + c * packed) for c in range(CHUNKS))
                    for n in range(CUTS)
                ]
            )[..., None],
            route_weight[:, k : k + 1],
            0.0,
        )
        for k, at in enumerate(chosen)
    )
    weights = jnp.concatenate(
        [weighted.astype(BF16), (weighted - lax.reduce_precision(weighted, 8, 7)).astype(BF16)], axis=1
    )
    row = jnp.arange(experts * part, dtype=jnp.int32)
    cuts = jnp.concatenate([(row // part * CUTS + n) * part + row % part for n in range(CUTS)])
    select = (cuts[:, None] == places).astype(BF16)
    place = (places[:, None] == cuts).astype(BF16)

    heads, mine_too = attend(
        queries, key_rows, value_rows, lambdas, head_gain, mine, lambda w: lax.ppermute(w, BOTH, sibling)
    )
    half = rows_local // 2
    heads = heads.reshape(2 * tp_size, half, 128)
    groups = [
        [s * tp_size + t for s in (n, sp_size - 1 - n) for t in range(tp_size)]
        for n in range(sp_size // 2)
    ]
    heads = lax.all_to_all(
        heads, BOTH, split_axis=0, concat_axis=0, tiled=True, axis_index_groups=groups
    ).reshape(2, tp_size, half, 128)
    heads = jnp.where(low, heads, heads[::-1])

    rest, heads = lax.optimization_barrier((down[later:], heads))
    rest = lax.ppermute(rest, BOTH, along)
    attended, *outgoing = project(heads, out_weight, stream, ffn_gain, dispatch)

    passed, outgoing = lax.optimization_barrier((passed, outgoing))
    passed_too = tuple(lax.ppermute(w, BOTH, sibling) for w in passed)
    rest_too = lax.ppermute(rest, BOTH, sibling)
    sets = (mine, mine_too, passed + (rest,), passed_too + (rest_too,))

    ring = tp_size // 2
    members = [
        [
            s * tp_size + (y + h * (ring // SHARERS)) * 2 + c
            for h in range(SHARERS)
            for s in range(sp_size)
        ]
        for y in range(ring // SHARERS)
        for c in range(2)
    ]

    def exchange(x):
        x = x.reshape(SHARERS * experts, CUTS * part, width // CUTS)
        return lax.all_to_all(
            x, BOTH, split_axis=0, concat_axis=0, tiled=True, axis_index_groups=members
        ).reshape(SHARERS, packed, width // CUTS)

    arrived = []
    for x in outgoing:
        arrived.append(exchange(x))
    returned = [exchange(expert(x, select, place, sets)) for x in arrived]
    return combine(returned, weights, attended)


def solution(mesh):
    placed = (
        P("sp", "tp"),
        P("sp", "tp"),
        P("sp", "tp"),
        P("tp"),
        P(),
        P(),
        P(("sp", "tp"), None),
        P(),
        P(("sp", "tp"), None),
        P(("sp", "tp"), None),
        P("sp", None, "tp"),
        P("sp", None, "tp"),
        P("sp", "tp", None),
    )
    return jax.shard_map(
        local, mesh=mesh, in_specs=placed, out_specs=P(("sp", "tp"), None), check_vma=False
    )
```

```python
import math

import jax
import jax.numpy as jnp
from jax import lax
from jax.experimental import pallas as pl
from jax.experimental.pallas import tpu as pltpu
from jax.sharding import PartitionSpec as P


DH = 64
PIECE = 512
ROWS = 256
SCALE = DH**-0.5 * math.log2(math.e)
BOTH = ("sp", "tp")
F32 = jnp.float32
BF16 = jnp.bfloat16
VMEM_LIMIT = 58 * 1024 * 1024
ATTENTION_LIMIT = 26 * 1024 * 1024
CHUNKS = 2
CUTS = 4
SHARERS = 2
FLOPS_US = 1.0e9


def dot(a, b, dims=((1,), (0,))):
    return lax.dot_general(a, b, (dims, ((), ())), preferred_element_type=F32)


def attention_body(pieces, side, first, final, count, *refs):
    sp_ref, lam_ref, gain_ref, q_ref = refs[:4]
    kv_refs, refs = refs[4 : 4 + count], refs[4 + count :]
    if first:
        m_ref, acc_ref = None, None
    else:
        (m_ref, acc_ref), refs = refs[:2], refs[2:]
    if final:
        (o_ref, m_sc, acc_sc), refs = refs[:3], refs[3:]
    else:
        (m_sc, acc_sc), refs = refs[:2], refs[2:]
    kv, sem, order, base_at, bounds = refs[:5]
    sp = sp_ref[0]
    z, x = sp // side, sp % side
    blocks = side * side
    begin = 0
    copies = []
    for n, ref in enumerate(kv_refs):
        copies.append(pltpu.make_async_copy(ref, kv.at[pl.ds(begin, ref.shape[0])], sem.at[n]))
        begin += ref.shape[0]
    for c in copies:
        c.start()
    if first:
        m_sc[...] = jnp.full(m_sc.shape, -1e30, F32)
        acc_sc[...] = jnp.zeros(acc_sc.shape, F32)
    else:
        m_sc[...] = m_ref[...]
        acc_sc[...] = acc_ref[...]

    mine = (blocks - 1 - sp, sp)
    for n, (dz, dx, low) in enumerate(pieces):
        block = (z + dz + side) % side * side + (x + dx + side) % side
        base_at[n] = block * (2 * PIECE) + low * PIECE
        for h in range(2):
            spot = jnp.int32(0) if n == 0 else bounds[h]
            order[h, spot] = jnp.int32(n)
            bounds[h] = spot + (block < mine[h]).astype(jnp.int32)
    for h in range(2):
        spot = bounds[h]
        for n in range(len(pieces)):
            order[h, spot] = jnp.int32(n)
            spot = spot + (base_at[n] // (2 * PIECE) == mine[h]).astype(jnp.int32)
        bounds[2 + h] = spot
    for c in copies:
        c.wait()

    rows = q_ref.shape[2]

    def step(h, at, masked):
        keys = len(at) * PIECE

        def operands():
            parts = [kv[pl.ds(pl.multiple_of(p * PIECE, PIECE), PIECE), :] for p in at]
            v = jnp.concatenate([p[:, 128:] for p in parts], axis=0)
            return (
                jnp.concatenate([p[:, :128] for p in parts], axis=0),
                jnp.concatenate([v, jnp.ones((keys, 128), BF16)], axis=1),
            )

        def tile(r):
            return pl.ds(r * ROWS if isinstance(r, int) else pl.multiple_of(r * ROWS, ROWS), ROWS)

        def scores(m, r, k):
            s = dot(q_ref[h, m, tile(r), :], k, ((1,), (1,)))
            if masked:
                row = r * ROWS + lax.broadcasted_iota(jnp.int32, s.shape, 0)
                start = jnp.where(h == 0, (blocks - 1 - sp) * (2 * PIECE) + 64, sp * (2 * PIECE))
                q_at = start + lax.shift_right_logical(row, 6) * 128 + (row & 63)
                key = lax.broadcasted_iota(jnp.int32, s.shape, 1)
                key = key + jnp.where(key < PIECE, base_at[at[0]], base_at[at[-1]] - (keys - PIECE))
                s = jnp.where(key <= q_at, s, -1e30)
            return s

        def finish(m, r, s, v):
            to = tile(r)
            old = m_sc[h, m, to, :]
            new = jnp.maximum(old, jnp.max(s, axis=1, keepdims=True))
            m_sc[h, m, to, :] = new
            p = jnp.exp2((s - jnp.concatenate([new] * (keys // 128), axis=1)) * SCALE)
            factor = jnp.exp2((old - new) * SCALE)
            both = jnp.concatenate([factor, factor], axis=1)
            acc_sc[h, m, to, :] = acc_sc[h, m, to, :] * both + dot(p.astype(BF16), v)

        def run(tiles):
            k, v = operands()
            s = scores(*tiles[0], k)
            for n, at_tile in enumerate(tiles):
                after = scores(*tiles[n + 1], k) if n + 1 < len(tiles) else None
                finish(*at_tile, s, v)
                s = after

        if len(at) == 2 and not masked:
            run([(m, r) for r in range(rows // ROWS) for m in range(2)])
        else:

            def some(r, carry):
                run([(m, r) for m in range(2)])
                return carry

            lax.fori_loop(0, rows // ROWS, some, 0)

    def half(h, carry):
        number = bounds[h]

        def pair(n, inner):
            step(h, (order[h, 2 * n], order[h, 2 * n + 1]), False)
            return inner

        lax.fori_loop(0, number // 2, pair, 0)

        @pl.when(number % 2 == 1)
        def _():
            step(h, (order[h, number - 1],), False)

        if not final:

            @pl.when(bounds[2 + h] > number)
            def _():
                step(h, (order[h, number], order[h, number + 1]), True)

        return carry

    lax.fori_loop(0, 2, half, 0)
    if final:
        def close(h, carry):
            c0 = acc_sc[h, 0, :, :128] / acc_sc[h, 0, :, 128:]
            c1 = acc_sc[h, 1, :, :128] / acc_sc[h, 1, :, 128:]
            c = c0 - lam_ref[0] * c1
            c = c * lax.rsqrt(jnp.mean(c * c, axis=1, keepdims=True) + 1e-05) * gain_ref[...]
            o_ref[jnp.where(sp < blocks // 2, 1 - h, h)] = c.astype(BF16)
            return carry

        lax.fori_loop(0, 2, close, 0)


def attention(q, arrays, pieces, state, lambdas, gain, sp, side, final):
    half = q.shape[2]
    first = state is None
    whole = pl.BlockSpec(memory_space=pltpu.VMEM)
    scalar = pl.BlockSpec(memory_space=pltpu.SMEM)
    held = (
        jax.ShapeDtypeStruct((2, 2, half, 128), F32),
        jax.ShapeDtypeStruct((2, 2, half, 256), F32),
    )
    scratch = [
        pltpu.VMEM((len(pieces) * PIECE, arrays[0].shape[1]), BF16),
        pltpu.SemaphoreType.DMA((len(arrays),)),
        pltpu.SMEM((2, len(pieces) + 2), jnp.int32),
        pltpu.SMEM((len(pieces),), jnp.int32),
        pltpu.SMEM((4,), jnp.int32),
    ]
    if final:
        scratch = [pltpu.VMEM(h.shape, F32) for h in held] + scratch
    return pl.pallas_call(
        lambda *refs: attention_body(pieces, side, first, final, len(arrays), *refs),
        in_specs=[scalar, scalar, whole, whole]
        + [pl.BlockSpec(memory_space=pl.ANY)] * len(arrays)
        + ([] if first else [whole, whole]),
        out_specs=whole if final else (whole, whole),
        out_shape=jax.ShapeDtypeStruct((2, half, 128), BF16) if final else held,
        scratch_shapes=scratch,
        compiler_params=pltpu.CompilerParams(vmem_limit_bytes=ATTENTION_LIMIT),
        cost_estimate=cost(len(pieces)),
        name="attention",
    )(sp.reshape(1), lambdas, gain.reshape(1, 128), q, *arrays, *(() if first else state))


def spread(array, forth, back):
    half = array.shape[0] // 2
    before, behind = lax.ppermute(array, "sp", forth), lax.ppermute(array, "sp", back)
    far = lax.ppermute(before[:half], "sp", forth), lax.ppermute(behind[half:], "sp", back)
    return (before, behind), far


def attend(queries, key_rows, value_rows, lambdas, head_gain, weights, later):
    sp_size, tp_size = lax.axis_size("sp"), lax.axis_size("tp")
    side = math.isqrt(sp_size)
    sp = lax.axis_index("sp")
    length = queries.shape[0]
    kv = jnp.concatenate([key_rows, value_rows], axis=1)
    ring = {}
    for name, dz, dx in (("z+", 1, 0), ("z-", -1, 0), ("x+", 0, 1), ("x-", 0, -1)):
        ring[name] = [
            (s, (s // side + dz) % side * side + (s % side + dx) % side) for s in range(sp_size)
        ]
    along_z, along_x = (ring["z+"], ring["z-"]), (ring["x+"], ring["x-"])
    upper, lower = kv[: length // 2], kv[length // 2 :]
    split = queries.reshape(tp_size, 2, length // (2 * tp_size), queries.shape[1])
    own = split[:, 0].reshape(length // 2, -1)
    near_u, far_u = spread(upper, *along_x)
    near_l, far_l = spread(lower, *along_z)
    other = lax.ppermute(
        split[:, 1].reshape(length // 2, -1), "sp", [(s, sp_size - 1 - s) for s in range(sp_size)]
    )
    row = jnp.concatenate([upper, *near_u, *far_u], axis=0)
    column = jnp.concatenate([lower, *near_l, *far_l], axis=0)
    near_row, far_row = spread(row, *along_z)
    near_column, far_column = spread(column, *along_x)
    steps = (0, -1, 1, 2)

    zero = jnp.zeros((2, length // 2, DH), BF16)
    q = jnp.stack([other, own])
    q = jnp.stack(
        [jnp.concatenate([q[..., :DH], zero], -1), jnp.concatenate([zero, q[..., DH:]], -1)], 1
    )
    calls = (
        ((row, column), [(0, d, 0) for d in steps] + [(d, 0, 1) for d in steps]),
        (
            near_row + near_column,
            [(e, d, 0) for e in (-1, 1) for d in steps] + [(d, e, 1) for e in (-1, 1) for d in steps],
        ),
        (far_row + far_column, [(2, d, 0) for d in steps] + [(d, 2, 1) for d in steps]),
    )
    state = None
    for n, (arrays, pieces) in enumerate(calls):
        state = attention(
            q, arrays, pieces, state, lambdas, head_gain, sp, side, n + 1 == len(calls)
        )
        if n == 0:
            weights, state = lax.optimization_barrier((weights, state))
            moved_late = later(weights)
    return state, moved_late


def project_body(h_ref, w_ref, s_ref, g_ref, d_ref, a_ref, *o_refs):
    parts = [jnp.concatenate([h_ref[n, t] for t in range(h_ref.shape[1])], axis=1) for n in range(2)]
    x = jnp.concatenate(parts, axis=0)
    attended = s_ref[...].astype(F32) + dot(x, w_ref[...])
    a_ref[...] = attended
    mean = jnp.mean(attended * attended, axis=1, keepdims=True)
    normed = (attended * lax.rsqrt(mean + 1e-06) * g_ref[...]).astype(BF16)
    pieces = stacked(normed)
    for c, o_ref in enumerate(o_refs):
        rows = dot(d_ref[c], pieces).astype(BF16)
        for h in range(SHARERS):
            o_ref[h] = rows


def stacked(x):
    wide = x.shape[1] // CUTS
    return jnp.concatenate([x[:, n * wide : (n + 1) * wide] for n in range(CUTS)], axis=0)


def project(heads, out_weight, stream, gain, dispatch):
    rows, width = stream.shape
    packed = jax.ShapeDtypeStruct((SHARERS, dispatch.shape[1], width // CUTS), BF16)
    return pl.pallas_call(
        project_body,
        out_shape=(jax.ShapeDtypeStruct((rows, width), F32),) + (packed,) * CHUNKS,
        compiler_params=pltpu.CompilerParams(vmem_limit_bytes=VMEM_LIMIT),
        cost_estimate=cost(5),
        name="project",
    )(heads, out_weight, stream, gain.reshape(1, width), dispatch)


def cost(microseconds):
    return pl.CostEstimate(flops=int(microseconds * FLOPS_US), bytes_accessed=0, transcendentals=0)


def expert_body(sizes, r_any, s_any, p_any, *refs):
    sets = len(sizes)
    flat, weights = refs, []
    for size in sizes:
        weights.append((flat[0], flat[1], flat[2:size]))
        flat = flat[size:]
    o_ref, r_ref, s_ref, p_ref, x_sc, act_sc, acc_sc, in_buf, down_buf, sem, small = flat
    hidden = in_buf.shape[2] // 2
    rows = s_ref.shape[0] // CUTS

    def start(n, kind):
        if kind < 2:
            to = in_buf.at[n, :, pl.ds(kind * hidden, hidden)]
            pltpu.make_async_copy(weights[n][kind], to, sem.at[3 * n + kind]).start()
        else:
            begin = n % 2 * hidden
            for piece in weights[n][2]:
                to = down_buf.at[n // 2, pl.ds(begin, piece.shape[0]), :]
                pltpu.make_async_copy(piece, to, sem.at[3 * n + 2]).start()
                begin += piece.shape[0]

    def share(h):
        return pl.ds(pl.multiple_of(h * rows, 16), rows)

    def landed(kind, n):
        if kind < 2:
            to = in_buf.at[n, :, pl.ds(kind * hidden, hidden)]
        else:
            to = down_buf.at[n // 2, pl.ds(pl.multiple_of(n % 2 * hidden, 128), hidden), :]
        pltpu.make_async_copy((weights[0][0], weights[0][1], weights[0][2][0])[kind], to, sem.at[3 * n + kind]).wait()

    first = pltpu.make_async_copy(r_any, r_ref, small.at[0])
    second = pltpu.make_async_copy(s_any, s_ref, small.at[1])
    third = pltpu.make_async_copy(p_any, p_ref, small.at[2])
    order = [
        (2 * p + n, kind)
        for p in range(sets // 2)
        for n, kind in ((0, 0), (0, 1), (1, 0), (1, 1), (0, 2), (1, 2))
    ]
    first.start()
    second.start()
    for n, kind in order[:2]:
        start(n, kind)
    first.wait()
    second.wait()
    for n, kind in order[2:]:
        start(n, kind)
    third.start()
    wide = r_ref.shape[2]

    def unpack(h, carry):
        cuts = dot(s_ref[...], r_ref[h]).astype(BF16)
        for n in range(CUTS):
            x_sc[share(h), n * wide : (n + 1) * wide] = cuts[n * rows : (n + 1) * rows]
        return carry

    lax.fori_loop(0, SHARERS, unpack, 0)

    def pair(p, carry):
        def one(v, inner):
            n = 2 * p + v
            for kind in range(2):
                landed(kind, n)
            both = dot(x_sc[...], in_buf[n])
            gate, upper = both[:, :hidden], both[:, hidden:]
            act = (gate / (1.0 + jnp.exp(-gate)) * upper).astype(BF16)
            act_sc[:, pl.ds(pl.multiple_of(v * hidden, 128), hidden)] = act
            return inner

        lax.fori_loop(0, 2, one, 0)
        landed(2, 2 * p)
        landed(2, 2 * p + 1)
        acc_sc[...] += dot(act_sc[...], down_buf[p])
        return carry

    acc_sc[...] = jnp.zeros(acc_sc.shape, F32)
    lax.fori_loop(0, sets // 2, pair, 0)
    third.wait()

    def repack(h, carry):
        o_ref[h] = dot(p_ref[...], stacked(acc_sc[share(h), :].astype(BF16))).astype(BF16)
        return carry

    lax.fori_loop(0, SHARERS, repack, 0)


def expert(arrived, select, place, sets):
    rows = SHARERS * select.shape[0] // CUTS
    width, hidden = sets[0][0].shape
    flat = [w for one in sets for w in one]
    return pl.pallas_call(
        lambda *refs: expert_body([len(one) for one in sets], *refs),
        in_specs=[pl.BlockSpec(memory_space=pl.ANY)] * (3 + len(flat)),
        out_specs=pl.BlockSpec(memory_space=pltpu.VMEM),
        out_shape=jax.ShapeDtypeStruct(arrived.shape, BF16),
        scratch_shapes=[
            pltpu.VMEM(arrived.shape, BF16),
            pltpu.VMEM(select.shape, BF16),
            pltpu.VMEM(place.shape, BF16),
            pltpu.VMEM((rows, width), BF16),
            pltpu.VMEM((rows, 2 * hidden), BF16),
            pltpu.VMEM((rows, width), F32),
            pltpu.VMEM((len(sets), width, 2 * hidden), BF16),
            pltpu.VMEM((len(sets) // 2, 2 * hidden, width), BF16),
            pltpu.SemaphoreType.DMA((3 * len(sets),)),
            pltpu.SemaphoreType.DMA((3,)),
        ],
        compiler_params=pltpu.CompilerParams(vmem_limit_bytes=VMEM_LIMIT),
        cost_estimate=cost(16),
        name="expert",
    )(arrived, select, place, *flat)


def halves_body(w_any, a_any, b_any, sem):
    rows = a_any.shape[0]
    first = pltpu.make_async_copy(w_any.at[pl.ds(0, rows)], a_any, sem.at[0])
    second = pltpu.make_async_copy(w_any.at[pl.ds(rows, rows)], b_any, sem.at[1])
    first.start()
    second.start()
    first.wait()
    second.wait()


def halves(w):
    out = jax.ShapeDtypeStruct((w.shape[0] // 2, w.shape[1]), w.dtype)
    return pl.pallas_call(
        halves_body,
        in_specs=[pl.BlockSpec(memory_space=pl.ANY)],
        out_specs=[pl.BlockSpec(memory_space=pltpu.HBM)] * 2,
        out_shape=[out, out],
        scratch_shapes=[pltpu.SemaphoreType.DMA((2,))],
        name="halves",
    )(w)


def combine_body(*refs):
    r_refs, (w_ref, a_ref, o_ref, r_sc) = refs[:CHUNKS], refs[CHUNKS:]
    wide = r_refs[0].shape[2]
    rows = a_ref.shape[0]
    for c, r_ref in enumerate(r_refs):
        total = sum(r_ref[h].astype(F32) for h in range(SHARERS))
        r_sc[c * total.shape[0] : (c + 1) * total.shape[0], :] = total.astype(BF16)

    def one(n, carry):
        at = pl.ds(pl.multiple_of(n * wide, 128), wide)
        both = dot(w_ref[n], r_sc[...])
        o_ref[:, at] = (a_ref[:, at] + (both[:rows] + both[rows:])).astype(BF16)
        return carry

    lax.fori_loop(0, CUTS, one, 0)


def combine(returned, weights, attended):
    return pl.pallas_call(
        combine_body,
        out_shape=jax.ShapeDtypeStruct(attended.shape, BF16),
        scratch_shapes=[pltpu.VMEM((weights.shape[2], attended.shape[1] // CUTS), BF16)],
        compiler_params=pltpu.CompilerParams(vmem_limit_bytes=VMEM_LIMIT),
        name="combine",
    )(*returned, weights, attended)


def moved(sp_size, tp_size, shift, flip):
    pairs = []
    for s in range(sp_size):
        for t in range(tp_size):
            y, c = t // 2, t % 2
            to = (y + shift(c)) % (tp_size // 2) * 2 + (c ^ flip)
            pairs.append((s * tp_size + t, s * tp_size + to))
    return pairs


def local(
    queries,
    key_rows,
    value_rows,
    lambdas,
    head_gain,
    out_weight,
    stream,
    ffn_gain,
    routes,
    route_weight,
    gate_weight,
    up_weight,
    down_weight,
):
    sp_size = lax.axis_size("sp")
    tp_size = lax.axis_size("tp")
    sp = lax.axis_index("sp")
    rows_local, width = stream.shape
    experts = sp_size * gate_weight.shape[0]
    top_count = routes.shape[1]
    low = sp < sp_size // 2

    mine = (gate_weight[0], up_weight[0], down_weight[0])
    along = moved(sp_size, tp_size, lambda c: 2 * c - 1, 0)
    sibling = moved(sp_size, tp_size, lambda c: 0, 1)
    passed = []
    passed = []
    for w in mine[:2]:
        passed.append(lax.ppermute(w, BOTH, along))

    def later(weights):
        soon, rest = halves(weights[2])
        soon = lax.ppermute(soon, BOTH, along)
        return tuple(lax.ppermute(w, BOTH, sibling) for w in weights), soon, rest

    slots = max(2, (rows_local * top_count * 5 + 4 * experts - 1) // (4 * experts))
    part = slots // CHUNKS
    flat = routes.reshape(-1)
    onehot = (flat[:, None] == jnp.arange(experts, dtype=jnp.int32)[None, :]).astype(BF16)
    count = flat.shape[0]
    earlier = (jnp.arange(count)[None, :] < jnp.arange(count)[:, None]).astype(BF16)
    slot = jnp.sum(dot(earlier, onehot) * onehot.astype(F32), axis=1).astype(jnp.int32)
    packed = experts * part * CUTS
    places = jnp.arange(packed, dtype=jnp.int32)

    def spots(k):
        e, j = (v.reshape(rows_local, top_count)[:, k] for v in (flat, slot))
        return [
            [jnp.where(j // part == c, (e * CUTS + n) * part + j % part, -1) for n in range(CUTS)]
            for c in range(CHUNKS)
        ]

    chosen = [spots(k) for k in range(top_count)]
    dispatch = sum(
        (places[:, None] == jnp.stack([jnp.concatenate(c) for c in at])[:, None, :]).astype(BF16)
        for at in chosen
    )
    every = jnp.arange(CHUNKS * packed, dtype=jnp.int32)
    weighted = sum(
        jnp.where(
            every
            == jnp.stack(
                [
                    sum(jnp.where(at[c][n] < 0, 0, at[c][n] + c * packed) for c in range(CHUNKS))
                    for n in range(CUTS)
                ]
            )[..., None],
            route_weight[:, k : k + 1],
            0.0,
        )
        for k, at in enumerate(chosen)
    )
    weights = jnp.concatenate(
        [weighted.astype(BF16), (weighted - lax.reduce_precision(weighted, 8, 7)).astype(BF16)], axis=1
    )
    row = jnp.arange(experts * part, dtype=jnp.int32)
    cuts = jnp.concatenate([(row // part * CUTS + n) * part + row % part for n in range(CUTS)])
    select = (cuts[:, None] == places).astype(BF16)
    place = (places[:, None] == cuts).astype(BF16)

    heads, (mine_too, soon, rest) = attend(
        queries, key_rows, value_rows, lambdas, head_gain, mine, later
    )
    passed = tuple(passed) + (soon,)
    half = rows_local // 2
    heads = heads.reshape(2 * tp_size, half, 128)
    groups = [
        [s * tp_size + t for s in (n, sp_size - 1 - n) for t in range(tp_size)]
        for n in range(sp_size // 2)
    ]
    heads = lax.all_to_all(
        heads, BOTH, split_axis=0, concat_axis=0, tiled=True, axis_index_groups=groups
    ).reshape(2, tp_size, half, 128)
    heads = jnp.where(low, heads, heads[::-1])

    rest, heads = lax.optimization_barrier((rest, heads))
    rest = lax.ppermute(rest, BOTH, along)
    attended, *outgoing = project(heads, out_weight, stream, ffn_gain, dispatch)

    passed, outgoing = lax.optimization_barrier((passed, outgoing))
    passed_too = tuple(lax.ppermute(w, BOTH, sibling) for w in passed)
    rest_too = lax.ppermute(rest, BOTH, sibling)
    sets = (mine, mine_too, passed + (rest,), passed_too + (rest_too,))

    ring = tp_size // 2
    members = [
        [
            s * tp_size + (y + h * (ring // SHARERS)) * 2 + c
            for h in range(SHARERS)
            for s in range(sp_size)
        ]
        for y in range(ring // SHARERS)
        for c in range(2)
    ]

    def exchange(x):
        x = x.reshape(SHARERS * experts, CUTS * part, width // CUTS)
        return lax.all_to_all(
            x, BOTH, split_axis=0, concat_axis=0, tiled=True, axis_index_groups=members
        ).reshape(SHARERS, packed, width // CUTS)

    arrived = []
    for x in outgoing:
        arrived.append(exchange(x))
    returned = [exchange(expert(x, select, place, sets)) for x in arrived]
    return combine(returned, weights, attended)


def solution(mesh):
    placed = (
        P("sp", "tp"),
        P("sp", "tp"),
        P("sp", "tp"),
        P("tp"),
        P(),
        P(),
        P(("sp", "tp"), None),
        P(),
        P(("sp", "tp"), None),
        P(("sp", "tp"), None),
        P("sp", None, "tp"),
        P("sp", None, "tp"),
        P("sp", "tp", None),
    )
    return jax.shard_map(
        local, mesh=mesh, in_specs=placed, out_specs=P(("sp", "tp"), None), check_vma=False
    )
```

```python
import math

import jax
import jax.numpy as jnp
from jax import lax
from jax.experimental import pallas as pl
from jax.experimental.pallas import tpu as pltpu
from jax.sharding import PartitionSpec as P


DH = 64
PIECE = 512
ROWS = 256
SCALE = DH**-0.5 * math.log2(math.e)
BOTH = ("sp", "tp")
F32 = jnp.float32
BF16 = jnp.bfloat16
VMEM_LIMIT = 56 * 1024 * 1024
ATTENTION_LIMIT = 26 * 1024 * 1024
CHUNKS = 2
CUTS = 4
SHARERS = 2
FLOPS_US = 1.0e9


def dot(a, b, dims=((1,), (0,))):
    return lax.dot_general(a, b, (dims, ((), ())), preferred_element_type=F32)


def attention_body(pieces, side, first, final, count, *refs):
    sp_ref, lam_ref, gain_ref, q_ref = refs[:4]
    kv_refs, refs = refs[4 : 4 + count], refs[4 + count :]
    if first:
        m_ref, acc_ref = None, None
    else:
        (m_ref, acc_ref), refs = refs[:2], refs[2:]
    if final:
        (o_ref, m_sc, acc_sc), refs = refs[:3], refs[3:]
    else:
        (m_sc, acc_sc), refs = refs[:2], refs[2:]
    kv, sem, order, base_at, bounds = refs[:5]
    sp = sp_ref[0]
    z, x = sp // side, sp % side
    blocks = side * side
    begin = 0
    copies = []
    for n, ref in enumerate(kv_refs):
        copies.append(pltpu.make_async_copy(ref, kv.at[pl.ds(begin, ref.shape[0])], sem.at[n]))
        begin += ref.shape[0]
    for c in copies:
        c.start()
    if first:
        m_sc[...] = jnp.full(m_sc.shape, -1e30, F32)
        acc_sc[...] = jnp.zeros(acc_sc.shape, F32)
    else:
        m_sc[...] = m_ref[...]
        acc_sc[...] = acc_ref[...]

    mine = (blocks - 1 - sp, sp)
    for n, (dz, dx, low) in enumerate(pieces):
        block = (z + dz + side) % side * side + (x + dx + side) % side
        base_at[n] = block * (2 * PIECE) + low * PIECE
        for h in range(2):
            spot = jnp.int32(0) if n == 0 else bounds[h]
            order[h, spot] = jnp.int32(n)
            bounds[h] = spot + (block < mine[h]).astype(jnp.int32)
    for h in range(2):
        spot = bounds[h]
        for n in range(len(pieces)):
            order[h, spot] = jnp.int32(n)
            spot = spot + (base_at[n] // (2 * PIECE) == mine[h]).astype(jnp.int32)
        bounds[2 + h] = spot
    for c in copies:
        c.wait()

    rows = q_ref.shape[2]

    def step(h, at, masked):
        keys = len(at) * PIECE

        def operands():
            parts = [kv[pl.ds(pl.multiple_of(p * PIECE, PIECE), PIECE), :] for p in at]
            v = jnp.concatenate([p[:, 128:] for p in parts], axis=0)
            return (
                jnp.concatenate([p[:, :128] for p in parts], axis=0),
                jnp.concatenate([v, jnp.ones((keys, 128), BF16)], axis=1),
            )

        def tile(r):
            return pl.ds(r * ROWS if isinstance(r, int) else pl.multiple_of(r * ROWS, ROWS), ROWS)

        def scores(m, r, k):
            s = dot(q_ref[h, m, tile(r), :], k, ((1,), (1,)))
            if masked:
                row = r * ROWS + lax.broadcasted_iota(jnp.int32, s.shape, 0)
                start = jnp.where(h == 0, (blocks - 1 - sp) * (2 * PIECE) + 64, sp * (2 * PIECE))
                q_at = start + lax.shift_right_logical(row, 6) * 128 + (row & 63)
                key = lax.broadcasted_iota(jnp.int32, s.shape, 1)
                key = key + jnp.where(key < PIECE, base_at[at[0]], base_at[at[-1]] - (keys - PIECE))
                s = jnp.where(key <= q_at, s, -1e30)
            return s

        def finish(m, r, s, v):
            to = tile(r)
            old = m_sc[h, m, to, :]
            new = jnp.maximum(old, jnp.max(s, axis=1, keepdims=True))
            m_sc[h, m, to, :] = new
            p = jnp.exp2((s - jnp.concatenate([new] * (keys // 128), axis=1)) * SCALE)
            factor = jnp.exp2((old - new) * SCALE)
            both = jnp.concatenate([factor, factor], axis=1)
            acc_sc[h, m, to, :] = acc_sc[h, m, to, :] * both + dot(p.astype(BF16), v)

        def run(tiles):
            k, v = operands()
            s = scores(*tiles[0], k)
            for n, at_tile in enumerate(tiles):
                after = scores(*tiles[n + 1], k) if n + 1 < len(tiles) else None
                finish(*at_tile, s, v)
                s = after

        if len(at) == 2 and not masked:
            run([(m, r) for r in range(rows // ROWS) for m in range(2)])
        else:

            def some(r, carry):
                run([(m, r) for m in range(2)])
                return carry

            lax.fori_loop(0, rows // ROWS, some, 0)

    def half(h, carry):
        number = bounds[h]

        def pair(n, inner):
            step(h, (order[h, 2 * n], order[h, 2 * n + 1]), False)
            return inner

        lax.fori_loop(0, number // 2, pair, 0)

        @pl.when(number % 2 == 1)
        def _():
            step(h, (order[h, number - 1],), False)

        if not final:

            @pl.when(bounds[2 + h] > number)
            def _():
                step(h, (order[h, number], order[h, number + 1]), True)

        return carry

    lax.fori_loop(0, 2, half, 0)
    if final:
        def close(h, carry):
            c0 = acc_sc[h, 0, :, :128] / acc_sc[h, 0, :, 128:]
            c1 = acc_sc[h, 1, :, :128] / acc_sc[h, 1, :, 128:]
            c = c0 - lam_ref[0] * c1
            c = c * lax.rsqrt(jnp.mean(c * c, axis=1, keepdims=True) + 1e-05) * gain_ref[...]
            o_ref[jnp.where(sp < blocks // 2, 1 - h, h)] = c.astype(BF16)
            return carry

        lax.fori_loop(0, 2, close, 0)


def attention(q, arrays, pieces, state, lambdas, gain, sp, side, final):
    half = q.shape[2]
    first = state is None
    whole = pl.BlockSpec(memory_space=pltpu.VMEM)
    scalar = pl.BlockSpec(memory_space=pltpu.SMEM)
    held = (
        jax.ShapeDtypeStruct((2, 2, half, 128), F32),
        jax.ShapeDtypeStruct((2, 2, half, 256), F32),
    )
    scratch = [
        pltpu.VMEM((len(pieces) * PIECE, arrays[0].shape[1]), BF16),
        pltpu.SemaphoreType.DMA((len(arrays),)),
        pltpu.SMEM((2, len(pieces) + 2), jnp.int32),
        pltpu.SMEM((len(pieces),), jnp.int32),
        pltpu.SMEM((4,), jnp.int32),
    ]
    if final:
        scratch = [pltpu.VMEM(h.shape, F32) for h in held] + scratch
    return pl.pallas_call(
        lambda *refs: attention_body(pieces, side, first, final, len(arrays), *refs),
        in_specs=[scalar, scalar, whole, whole]
        + [pl.BlockSpec(memory_space=pl.ANY)] * len(arrays)
        + ([] if first else [whole, whole]),
        out_specs=whole if final else (whole, whole),
        out_shape=jax.ShapeDtypeStruct((2, half, 128), BF16) if final else held,
        scratch_shapes=scratch,
        compiler_params=pltpu.CompilerParams(vmem_limit_bytes=ATTENTION_LIMIT),
        cost_estimate=cost(len(pieces)),
        name="attention",
    )(sp.reshape(1), lambdas, gain.reshape(1, 128), q, *arrays, *(() if first else state))


def spread(array, forth, back):
    half = array.shape[0] // 2
    before, behind = lax.ppermute(array, "sp", forth), lax.ppermute(array, "sp", back)
    far = lax.ppermute(before[:half], "sp", forth), lax.ppermute(behind[half:], "sp", back)
    return (before, behind), far


def attend(queries, key_rows, value_rows, lambdas, head_gain, weights, swap):
    sp_size, tp_size = lax.axis_size("sp"), lax.axis_size("tp")
    side = math.isqrt(sp_size)
    sp = lax.axis_index("sp")
    length = queries.shape[0]
    kv = jnp.concatenate([key_rows, value_rows], axis=1)
    ring = {}
    for name, dz, dx in (("z+", 1, 0), ("z-", -1, 0), ("x+", 0, 1), ("x-", 0, -1)):
        ring[name] = [
            (s, (s // side + dz) % side * side + (s % side + dx) % side) for s in range(sp_size)
        ]
    along_z, along_x = (ring["z+"], ring["z-"]), (ring["x+"], ring["x-"])
    upper, lower = kv[: length // 2], kv[length // 2 :]
    split = queries.reshape(tp_size, 2, length // (2 * tp_size), queries.shape[1])
    own = split[:, 0].reshape(length // 2, -1)
    near_u, far_u = spread(upper, *along_x)
    near_l, far_l = spread(lower, *along_z)
    other = lax.ppermute(
        split[:, 1].reshape(length // 2, -1), "sp", [(s, sp_size - 1 - s) for s in range(sp_size)]
    )
    row = jnp.concatenate([upper, *near_u, *far_u], axis=0)
    column = jnp.concatenate([lower, *near_l, *far_l], axis=0)
    near_row, far_row = spread(row, *along_z)
    near_column, far_column = spread(column, *along_x)
    steps = (0, -1, 1, 2)

    zero = jnp.zeros((2, length // 2, DH), BF16)
    q = jnp.stack([other, own])
    q = jnp.stack(
        [jnp.concatenate([q[..., :DH], zero], -1), jnp.concatenate([zero, q[..., DH:]], -1)], 1
    )
    calls = (
        ((row, column), [(0, d, 0) for d in steps] + [(d, 0, 1) for d in steps]),
        (
            near_row + near_column,
            [(e, d, 0) for e in (-1, 1) for d in steps] + [(d, e, 1) for e in (-1, 1) for d in steps],
        ),
        (far_row + far_column, [(2, d, 0) for d in steps] + [(d, 2, 1) for d in steps]),
    )
    state = None
    for n, (arrays, pieces) in enumerate(calls):
        state = attention(
            q, arrays, pieces, state, lambdas, head_gain, sp, side, n + 1 == len(calls)
        )
        if n == 0:
            weights, state = lax.optimization_barrier((weights, state))
            swapped = tuple(swap(w) for w in weights)
    return state, swapped


def project_body(h_ref, w_ref, s_ref, g_ref, d_ref, a_ref, *o_refs):
    parts = [jnp.concatenate([h_ref[n, t] for t in range(h_ref.shape[1])], axis=1) for n in range(2)]
    x = jnp.concatenate(parts, axis=0)
    attended = s_ref[...].astype(F32) + dot(x, w_ref[...])
    a_ref[...] = attended
    mean = jnp.mean(attended * attended, axis=1, keepdims=True)
    normed = (attended * lax.rsqrt(mean + 1e-06) * g_ref[...]).astype(BF16)
    pieces = stacked(normed)
    for c, o_ref in enumerate(o_refs):
        rows = dot(d_ref[c], pieces).astype(BF16)
        for h in range(SHARERS):
            o_ref[h] = rows


def stacked(x):
    wide = x.shape[1] // CUTS
    return jnp.concatenate([x[:, n * wide : (n + 1) * wide] for n in range(CUTS)], axis=0)


def project(heads, out_weight, stream, gain, dispatch):
    rows, width = stream.shape
    packed = jax.ShapeDtypeStruct((SHARERS, dispatch.shape[1], width // CUTS), BF16)
    return pl.pallas_call(
        project_body,
        out_shape=(jax.ShapeDtypeStruct((rows, width), F32),) + (packed,) * CHUNKS,
        compiler_params=pltpu.CompilerParams(vmem_limit_bytes=ATTENTION_LIMIT),
        cost_estimate=cost(5),
        name="project",
    )(heads, out_weight, stream, gain.reshape(1, width), dispatch)


def cost(microseconds):
    return pl.CostEstimate(flops=int(microseconds * FLOPS_US), bytes_accessed=0, transcendentals=0)


def expert_body(sets, r_any, s_any, p_any, *refs):
    weights = refs[: 3 * sets]
    o_ref, r_ref, s_ref, p_ref, x_sc, act_sc, acc_sc, in_buf, down_buf, sem, small = refs[3 * sets :]
    hidden = in_buf.shape[2] // 2
    rows = s_ref.shape[0] // CUTS

    def copy(n, kind):
        if kind < 2:
            to = in_buf.at[n, :, pl.ds(kind * hidden, hidden)]
        else:
            to = down_buf.at[n // 2, pl.ds(n % 2 * hidden, hidden), :]
        return pltpu.make_async_copy(weights[3 * n + kind], to, sem.at[3 * n + kind])

    def share(h):
        return pl.ds(pl.multiple_of(h * rows, 16), rows)

    def landed(kind, n):
        if kind < 2:
            to = in_buf.at[n, :, pl.ds(kind * hidden, hidden)]
        else:
            to = down_buf.at[n // 2, pl.ds(pl.multiple_of(n % 2 * hidden, 128), hidden), :]
        pltpu.make_async_copy(weights[kind], to, sem.at[3 * n + kind]).wait()

    first = pltpu.make_async_copy(r_any, r_ref, small.at[0])
    second = pltpu.make_async_copy(s_any, s_ref, small.at[1])
    third = pltpu.make_async_copy(p_any, p_ref, small.at[2])
    order = [
        (2 * p + n, kind)
        for p in range(sets // 2)
        for n, kind in ((0, 0), (0, 1), (1, 0), (1, 1), (0, 2), (1, 2))
    ]
    first.start()
    second.start()
    for n, kind in order[:2]:
        copy(n, kind).start()
    first.wait()
    second.wait()
    for n, kind in order[2:]:
        copy(n, kind).start()
    third.start()
    wide = r_ref.shape[2]

    def unpack(h, carry):
        cuts = dot(s_ref[...], r_ref[h]).astype(BF16)
        for n in range(CUTS):
            x_sc[share(h), n * wide : (n + 1) * wide] = cuts[n * rows : (n + 1) * rows]
        return carry

    lax.fori_loop(0, SHARERS, unpack, 0)

    def pair(p, carry):
        def one(v, inner):
            n = 2 * p + v
            for kind in range(2):
                landed(kind, n)
            both = dot(x_sc[...], in_buf[n])
            gate, upper = both[:, :hidden], both[:, hidden:]
            act = (gate / (1.0 + jnp.exp(-gate)) * upper).astype(BF16)
            act_sc[:, pl.ds(pl.multiple_of(v * hidden, 128), hidden)] = act
            return inner

        lax.fori_loop(0, 2, one, 0)
        landed(2, 2 * p)
        landed(2, 2 * p + 1)
        acc_sc[...] += dot(act_sc[...], down_buf[p])
        return carry

    acc_sc[...] = jnp.zeros(acc_sc.shape, F32)
    lax.fori_loop(0, sets // 2, pair, 0)
    third.wait()

    def repack(h, carry):
        o_ref[h] = dot(p_ref[...], stacked(acc_sc[share(h), :].astype(BF16))).astype(BF16)
        return carry

    lax.fori_loop(0, SHARERS, repack, 0)


def expert(arrived, select, place, sets):
    rows = SHARERS * select.shape[0] // CUTS
    width, hidden = sets[0][0].shape
    flat = [w for one in sets for w in one]
    return pl.pallas_call(
        lambda *refs: expert_body(len(sets), *refs),
        in_specs=[pl.BlockSpec(memory_space=pl.ANY)] * (3 + len(flat)),
        out_specs=pl.BlockSpec(memory_space=pltpu.VMEM),
        out_shape=jax.ShapeDtypeStruct(arrived.shape, BF16),
        scratch_shapes=[
            pltpu.VMEM(arrived.shape, BF16),
            pltpu.VMEM(select.shape, BF16),
            pltpu.VMEM(place.shape, BF16),
            pltpu.VMEM((rows, width), BF16),
            pltpu.VMEM((rows, 2 * hidden), BF16),
            pltpu.VMEM((rows, width), F32),
            pltpu.VMEM((len(sets), width, 2 * hidden), BF16),
            pltpu.VMEM((len(sets) // 2, 2 * hidden, width), BF16),
            pltpu.SemaphoreType.DMA((len(flat),)),
            pltpu.SemaphoreType.DMA((3,)),
        ],
        compiler_params=pltpu.CompilerParams(vmem_limit_bytes=VMEM_LIMIT),
        cost_estimate=cost(16),
        name="expert",
    )(arrived, select, place, *flat)


def combine_body(*refs):
    r_refs, (w_ref, a_ref, o_ref, r_sc) = refs[:CHUNKS], refs[CHUNKS:]
    wide = r_refs[0].shape[2]
    rows = a_ref.shape[0]
    for c, r_ref in enumerate(r_refs):
        total = sum(r_ref[h].astype(F32) for h in range(SHARERS))
        r_sc[c * total.shape[0] : (c + 1) * total.shape[0], :] = total.astype(BF16)

    def one(n, carry):
        at = pl.ds(pl.multiple_of(n * wide, 128), wide)
        both = dot(w_ref[n], r_sc[...])
        o_ref[:, at] = (a_ref[:, at] + (both[:rows] + both[rows:])).astype(BF16)
        return carry

    lax.fori_loop(0, CUTS, one, 0)


def combine(returned, weights, attended):
    return pl.pallas_call(
        combine_body,
        out_shape=jax.ShapeDtypeStruct(attended.shape, BF16),
        scratch_shapes=[pltpu.VMEM((weights.shape[2], attended.shape[1] // CUTS), BF16)],
        compiler_params=pltpu.CompilerParams(vmem_limit_bytes=ATTENTION_LIMIT),
        name="combine",
    )(*returned, weights, attended)


def moved(sp_size, tp_size, shift, flip):
    pairs = []
    for s in range(sp_size):
        for t in range(tp_size):
            y, c = t // 2, t % 2
            to = (y + shift(c)) % (tp_size // 2) * 2 + (c ^ flip)
            pairs.append((s * tp_size + t, s * tp_size + to))
    return pairs


def local(
    queries,
    key_rows,
    value_rows,
    lambdas,
    head_gain,
    out_weight,
    stream,
    ffn_gain,
    routes,
    route_weight,
    gate_weight,
    up_weight,
    down_weight,
):
    sp_size = lax.axis_size("sp")
    tp_size = lax.axis_size("tp")
    sp = lax.axis_index("sp")
    rows_local, width = stream.shape
    experts = sp_size * gate_weight.shape[0]
    top_count = routes.shape[1]
    low = sp < sp_size // 2

    mine = (gate_weight[0], up_weight[0], down_weight[0])
    along = moved(sp_size, tp_size, lambda c: 2 * c - 1, 0)
    sibling = moved(sp_size, tp_size, lambda c: 0, 1)
    passed = []
    for w in mine:
        passed.append(lax.ppermute(w, BOTH, along))
    passed = tuple(passed)

    slots = max(2, (rows_local * top_count * 5 + 4 * experts - 1) // (4 * experts))
    part = slots // CHUNKS
    flat = routes.reshape(-1)
    onehot = (flat[:, None] == jnp.arange(experts, dtype=jnp.int32)[None, :]).astype(BF16)
    count = flat.shape[0]
    earlier = (jnp.arange(count)[None, :] < jnp.arange(count)[:, None]).astype(BF16)
    slot = jnp.sum(dot(earlier, onehot) * onehot.astype(F32), axis=1).astype(jnp.int32)
    packed = experts * part * CUTS
    places = jnp.arange(packed, dtype=jnp.int32)

    def spots(k):
        e, j = (v.reshape(rows_local, top_count)[:, k] for v in (flat, slot))
        return [
            [jnp.where(j // part == c, (e * CUTS + n) * part + j % part, -1) for n in range(CUTS)]
            for c in range(CHUNKS)
        ]

    chosen = [spots(k) for k in range(top_count)]
    dispatch = sum(
        (places[:, None] == jnp.stack([jnp.concatenate(c) for c in at])[:, None, :]).astype(BF16)
        for at in chosen
    )
    every = jnp.arange(CHUNKS * packed, dtype=jnp.int32)
    weighted = sum(
        jnp.where(
            every
            == jnp.stack(
                [
                    sum(jnp.where(at[c][n] < 0, 0, at[c][n] + c * packed) for c in range(CHUNKS))
                    for n in range(CUTS)
                ]
            )[..., None],
            route_weight[:, k : k + 1],
            0.0,
        )
        for k, at in enumerate(chosen)
    )
    weights = jnp.concatenate(
        [weighted.astype(BF16), (weighted - lax.reduce_precision(weighted, 8, 7)).astype(BF16)], axis=1
    )
    row = jnp.arange(experts * part, dtype=jnp.int32)
    cuts = jnp.concatenate([(row // part * CUTS + n) * part + row % part for n in range(CUTS)])
    select = (cuts[:, None] == places).astype(BF16)
    place = (places[:, None] == cuts).astype(BF16)

    heads, mine_too = attend(
        queries, key_rows, value_rows, lambdas, head_gain, mine, lambda w: lax.ppermute(w, BOTH, sibling)
    )
    half = rows_local // 2
    heads = heads.reshape(2 * tp_size, half, 128)
    groups = [
        [s * tp_size + t for s in (n, sp_size - 1 - n) for t in range(tp_size)]
        for n in range(sp_size // 2)
    ]
    heads = lax.all_to_all(
        heads, BOTH, split_axis=0, concat_axis=0, tiled=True, axis_index_groups=groups
    ).reshape(2, tp_size, half, 128)
    heads = jnp.where(low, heads, heads[::-1])

    attended, *outgoing = project(heads, out_weight, stream, ffn_gain, dispatch)

    passed, outgoing = lax.optimization_barrier((passed, outgoing))
    passed_too = tuple(lax.ppermute(w, BOTH, sibling) for w in passed)
    sets = (mine, mine_too, passed, passed_too)

    ring = tp_size // 2
    members = [
        [
            s * tp_size + (y + h * (ring // SHARERS)) * 2 + c
            for h in range(SHARERS)
            for s in range(sp_size)
        ]
        for y in range(ring // SHARERS)
        for c in range(2)
    ]

    def exchange(x):
        x = x.reshape(SHARERS * experts, CUTS * part, width // CUTS)
        return lax.all_to_all(
            x, BOTH, split_axis=0, concat_axis=0, tiled=True, axis_index_groups=members
        ).reshape(SHARERS, packed, width // CUTS)

    arrived = [exchange(x) for x in outgoing]
    returned = [exchange(expert(x, select, place, sets)) for x in arrived]
    return combine(returned, weights, attended)


def solution(mesh):
    placed = (
        P("sp", "tp"),
        P("sp", "tp"),
        P("sp", "tp"),
        P("tp"),
        P(),
        P(),
        P(("sp", "tp"), None),
        P(),
        P(("sp", "tp"), None),
        P(("sp", "tp"), None),
        P("sp", None, "tp"),
        P("sp", None, "tp"),
        P("sp", "tp", None),
    )
    return jax.shard_map(
        local, mesh=mesh, in_specs=placed, out_specs=P(("sp", "tp"), None), check_vma=False
    )
```
